512 devices in a mesh: grp: 2 (over y), fs: 32 (over z), tp: 8 (over x, core).
Axes of the slice: x: 4, y: 2, z: 32, core: 2. Of those that a mesh axis runs over, the one named last changes fastest.
The devices are a block of a 4x8x32 slice.
Arguments:
- prompt: bfloat16 [4096, 2048], P(('grp', 'tp')), parts along dimension 0, may hold values from -6 to 6
- gain_first: float32 [2048], P('fs'), may hold values from 0.1 to 1.9
- gate_first: float32 [2048, 4096], P('fs', 'tp'), may hold values from -0.125 to 0.125
- up_first: float32 [2048, 4096], P('fs', 'tp'), may hold values from -0.125 to 0.125
- down_first: float32 [4096, 2048], P('fs', 'tp'), may hold values from -0.09375 to 0.09375
- gain_second: float32 [2048], P('fs'), may hold values from 0.1 to 1.9
- gate_second: float32 [2048, 4096], P('fs', 'tp'), may hold values from -0.125 to 0.125
- up_second: float32 [2048, 4096], P('fs', 'tp'), may hold values from -0.125 to 0.125
- down_second: float32 [4096, 2048], P('fs', 'tp'), may hold values from -0.09375 to 0.09375
Outputs:
- result: bfloat16 [4096, 2048], P(('grp', 'tp')), parts along dimension 0
- served_gate_first: bfloat16 [4096, 4096], P('grp', 'fs'), parts along dimension 0
- served_up_first: bfloat16 [4096, 4096], P('grp', 'fs'), parts along dimension 0
- served_down_first: bfloat16 [4096, 4096], P('fs', 'grp'), parts along dimension 1
- served_gate_second: bfloat16 [4096, 4096], P('grp', 'fs'), parts along dimension 0
- served_up_second: bfloat16 [4096, 4096], P('grp', 'fs'), parts along dimension 0
- served_down_second: bfloat16 [4096, 4096], P('fs', 'grp'), parts along dimension 1
The draws below stay inside these ranges and needn't reach their ends.
There are 2 independent parts, one for each index of `grp`. The reference program is written for one: setup_inputs(seed, part) draws one part's arguments, and reference() takes and returns one part's arrays. A program takes and returns all parts, laid end to end along the dimension named above; an argument that names none is the same for every part. Nothing has to cross between parts.
All inputs are finite; a program needn't handle non-finite values.
Results may differ from the reference program's by a relative error of at most 0.0053.
Values may be sent and summed in bfloat16 or wider, within the bound.
No kernel may reach another device: no remote copies, remote signals or barrier semaphores. Data moves between devices by JAX's collectives and lax.ppermute only.
A program may use at most 64 MiB of HBM per device.

```python
import jax
import jax.numpy as jnp
from jax import lax

D = 2048
FF = 4096
TOKENS = 2048


def block_scale(rng, extent, shards, low, top_value):
    factor_of, own = 1.0, jax.random.fold_in(rng, 6)
    for position, blocks in shards:
        draws = jnp.exp(jax.random.uniform(jax.random.fold_in(own, position), (blocks,), jnp.float32, low / len(shards), top_value / len(shards)))
        factor_of = factor_of * jnp.repeat(draws, extent[position] // blocks).reshape([-1 if axis == position else 1 for axis in range(len(extent))])
    return factor_of


def gaussian(stream_key, dims, deviation, most, pieces=(), dtype=jnp.bfloat16):
    entries = deviation * jax.random.normal(stream_key, dims, jnp.float32)
    if pieces:
        entries = entries * block_scale(stream_key, dims, pieces, -0.22, 0.18)
    return jnp.clip(entries, -most, most).astype(dtype)


def setup_inputs(seed: int = 0, part: int = 0) -> dict:
    splits = jax.random.split(jax.random.key(seed), 10)
    own_keys = jax.random.split(jax.random.fold_in(splits[9], part), 10)
    return {
        "prompt": gaussian(own_keys[0], (TOKENS, D), 1.0, 6.0, ((0, 8),)),
        "gain_first": jnp.clip(1.0 + 0.18 * jax.random.normal(splits[1], (D,), jnp.float32), 0.1, 1.9),
        "gate_first": gaussian(splits[2], (D, FF), D ** -0.5, 0.125, ((0, 32), (1, 8)), jnp.float32),
        "up_first": gaussian(splits[3], (D, FF), D ** -0.5, 0.125, ((0, 32), (1, 8)), jnp.float32),
        "down_first": gaussian(splits[4], (FF, D), FF ** -0.5, 0.09375, ((0, 32), (1, 8)), jnp.float32),
        "gain_second": jnp.clip(1.0 + 0.18 * jax.random.normal(splits[5], (D,), jnp.float32), 0.1, 1.9),
        "gate_second": gaussian(splits[6], (D, FF), D ** -0.5, 0.125, ((0, 32), (1, 8)), jnp.float32),
        "up_second": gaussian(splits[7], (D, FF), D ** -0.5, 0.125, ((0, 32), (1, 8)), jnp.float32),
        "down_second": gaussian(splits[8], (FF, D), FF ** -0.5, 0.09375, ((0, 32), (1, 8)), jnp.float32),
    }


EPS = 1e-06

def fold(gain, weight):
    return (gain[:, None] * weight).astype(jnp.bfloat16)

def normed_of(stream):
    return (stream * lax.rsqrt(lax.optimization_barrier(jnp.mean(stream * stream, axis=-1, keepdims=True)) + EPS)).astype(jnp.bfloat16)

def block(stream, w_gate, w_up, w_down):
    normed = normed_of(stream)
    gate = jnp.dot(normed, w_gate, preferred_element_type=jnp.float32)
    up_val = jnp.dot(normed, w_up, preferred_element_type=jnp.float32)
    hidden = (jax.nn.silu(gate) * up_val).astype(jnp.bfloat16)
    return stream + 0.5 * jnp.dot(hidden, w_down, preferred_element_type=jnp.float32)

def reference(prompt, gain_first, gate_first, up_first, down_first, gain_second, gate_second, up_second, down_second):
    g_one = fold(gain_first, gate_first)
    u_one = fold(gain_first, up_first)
    d_one = down_first.astype(jnp.bfloat16)
    g_two = fold(gain_second, gate_second)
    u_two = fold(gain_second, up_second)
    d_two = down_second.astype(jnp.bfloat16)
    stream = prompt.astype(jnp.float32)
    stream = block(stream, g_one, u_one, d_one)
    stream = block(stream, g_two, u_two, d_two)
    return (stream.astype(jnp.bfloat16), g_one, u_one, d_one, g_two, u_two, d_two)
```

```python
import jax
import jax.numpy as jnp
from jax import lax
from jax.experimental.layout import Layout, with_layout_constraint
from jax.sharding import PartitionSpec as P

EPS = 1e-06
NEAR = 4
BF16 = jnp.bfloat16


def fold(gain, weight):
    return (gain[:, None] * weight).astype(BF16)


def normed_of(stream):
    return (stream * lax.rsqrt(jnp.mean(stream * stream, axis=-1, keepdims=True) + EPS)).astype(BF16)


def row_major(array):
    return with_layout_constraint(array, Layout(major_to_minor=tuple(range(array.ndim))))


def exchange(blocks, axis, groups=None):
    return lax.all_to_all(blocks, axis, split_axis=0, concat_axis=0, tiled=True, axis_index_groups=groups)


def spread_copies(array, axis, members, groups=None):
    return exchange(jnp.broadcast_to(array, (members, *array.shape)), axis, groups)


def near_groups(n):
    return [[NEAR * a + i for i in range(NEAR)] for a in range(n // NEAR)]


def far_groups(n):
    return [[i + NEAR * j for j in range(n // NEAR)] for i in range(NEAR)]


def chip_groups(n):
    return [list(range(c, n, 2)) for c in range(2)]


def gather_tp(array):
    n = lax.axis_size("tp")
    mine = spread_copies(array, "tp", n // 2, chip_groups(n))
    other = lax.ppermute(mine, "tp", [(i, i ^ 1) for i in range(n)])
    even = lax.axis_index("tp") % 2 == 0
    both = jnp.stack([jnp.where(even, mine, other), jnp.where(even, other, mine)], axis=1)
    return both.reshape(n, *array.shape)


def scatter_sum(partial):
    n = lax.axis_size("fs")
    far = n // NEAR
    rows = partial.shape[0] // n
    width = partial.shape[1]
    blocks = partial.astype(BF16).reshape(far, NEAR, rows, width).transpose(1, 0, 2, 3)
    got = exchange(blocks, "fs", near_groups(n))
    total = jnp.sum(got.astype(jnp.float32), axis=0).astype(BF16)
    got = exchange(total, "fs", far_groups(n))
    return jnp.sum(got.astype(jnp.float32), axis=0)


def gather_tokens(own):
    n = lax.axis_size("fs")
    far = n // NEAR
    rows, width = own.shape
    got = spread_copies(own, "fs", far, far_groups(n))
    got = spread_copies(got, "fs", NEAR, near_groups(n))
    return got.transpose(1, 0, 2, 3).reshape(n * rows, width)


def on_device(
    prompt,
    gain_first,
    gate_first,
    up_first,
    down_first,
    gain_second,
    gate_second,
    up_second,
    down_second,
):
    n_fs = lax.axis_size("fs")
    n_tp = lax.axis_size("tp")
    rows, cols = gate_first.shape
    hid, dcols = down_first.shape
    width = prompt.shape[1]
    half = cols // dcols

    g1, u1 = fold(gain_first, gate_first), fold(gain_first, up_first)
    g2, u2 = fold(gain_second, gate_second), fold(gain_second, up_second)
    d1, d2 = down_first.astype(BF16), down_second.astype(BF16)

    pack = [m[:, k * dcols : (k + 1) * dcols] for m in (g2, u2) for k in range(half)] + [d2]
    whole = lax.all_gather(row_major(jnp.concatenate(pack, axis=0)), "fs", axis=0, tiled=True)
    whole = row_major(whole).reshape(n_fs, 2 * half * rows + hid, dcols)

    r = rows // n_tp
    lanes = cols * n_tp // n_fs
    per = n_fs // n_tp
    mats = jnp.stack([g1, u1, g2, u2]).reshape(4, n_tp, r, cols).transpose(1, 0, 2, 3)
    mats = exchange(mats, "tp")
    mats = mats.reshape(n_tp, 4, r, per, lanes).transpose(0, 3, 1, 2, 4).reshape(n_fs, 4, r, lanes)
    mats = exchange(mats, "fs")

    def packed(pair, down):
        parts = [down[:, k * lanes : (k + 1) * lanes] for k in range(dcols // lanes)]
        return jnp.concatenate([pair.reshape(-1, lanes), *parts], axis=0)

    def served_of(got):
        pair = got[:, : 2 * n_fs * r].reshape(n_tp, n_fs, 2, r, lanes)
        pair = pair.transpose(2, 1, 0, 3, 4).reshape(2, width, lanes)
        down = got[:, 2 * n_fs * r :].reshape(n_tp, dcols // lanes, hid, lanes)
        down = down.transpose(2, 0, 1, 3).reshape(hid, width)
        return pair[0], pair[1], down

    first = served_of(gather_tp(packed(mats[:, :2], d1)))
    second = served_of(lax.all_gather(packed(mats[:, 2:], d2), "tp", axis=0, tiled=False))

    stream = prompt.astype(jnp.float32)
    normed = normed_of(stream)
    gate = jnp.dot(normed, first[0], preferred_element_type=jnp.float32)
    up = jnp.dot(normed, first[1], preferred_element_type=jnp.float32)
    hidden = (jax.nn.silu(gate) * up).astype(BF16)
    partial = jnp.dot(hidden, first[2], preferred_element_type=jnp.float32)
    tokens = prompt.shape[0] // n_fs
    own = lax.dynamic_slice_in_dim(prompt, lax.axis_index("fs") * tokens, tokens, 0).astype(jnp.float32)
    own = own + 0.5 * scatter_sum(partial)

    normed = spread_copies(normed_of(own), "tp", n_tp).reshape(n_tp * tokens, width)
    normed, whole = lax.optimization_barrier((normed, whole))

    def columns(m):
        parts = [whole[:, (m * half + k) * rows : (m * half + k + 1) * rows].reshape(width, dcols) for k in range(half)]
        return jnp.concatenate([jnp.dot(normed, w, preferred_element_type=jnp.float32) for w in parts], axis=1)

    hidden = (jax.nn.silu(columns(0)) * columns(1)).astype(BF16)
    hidden = spread_copies(hidden, "tp", n_tp)
    hidden = hidden.transpose(1, 0, 2).reshape(n_tp * tokens, n_tp * cols)
    down = whole[:, 2 * half * rows :].reshape(n_fs * hid, dcols)
    out = jnp.dot(hidden, down, preferred_element_type=jnp.float32)
    out = exchange(out.reshape(n_tp, tokens, dcols), "tp")
    own = own + 0.5 * out.transpose(1, 0, 2).reshape(tokens, width)
    result = gather_tokens(own.astype(BF16))
    return (result, first[0], first[1], first[2], second[0], second[1], second[2])


def solution(mesh):
    return jax.shard_map(
        on_device,
        mesh=mesh,
        in_specs=(
            P(("grp", "tp"), None),
            P("fs"),
            P("fs", "tp"),
            P("fs", "tp"),
            P("fs", "tp"),
            P("fs"),
            P("fs", "tp"),
            P("fs", "tp"),
            P("fs", "tp"),
        ),
        out_specs=(
            P(("grp", "tp"), None),
            P("grp", "fs"),
            P("grp", "fs"),
            P("fs", "grp"),
            P("grp", "fs"),
            P("grp", "fs"),
            P("fs", "grp"),
        ),
        check_vma=False,
    )
```

```python
import jax
import jax.numpy as jnp
from jax import lax
from jax.experimental.layout import Layout, with_layout_constraint
from jax.sharding import PartitionSpec as P

EPS = 1e-06
NEAR = 4
BF16 = jnp.bfloat16


def fold(gain, weight):
    return (gain[:, None] * weight).astype(BF16)


def normed_of(stream):
    return (stream * lax.rsqrt(jnp.mean(stream * stream, axis=-1, keepdims=True) + EPS)).astype(BF16)


def row_major(array):
    return with_layout_constraint(array, Layout(major_to_minor=tuple(range(array.ndim))))


def exchange(blocks, axis, groups=None):
    return lax.all_to_all(blocks, axis, split_axis=0, concat_axis=0, tiled=True, axis_index_groups=groups)


def spread_copies(array, axis, members, groups=None):
    return exchange(jnp.broadcast_to(array, (members, *array.shape)), axis, groups)


def far_groups(n):
    stride = 2 * NEAR
    return [list(range(i, n, stride)) for i in range(stride)]


def chip_groups(n):
    return [list(range(c, n, 2)) for c in range(2)]


def gather_tp(array):
    n = lax.axis_size("tp")
    mine = spread_copies(array, "tp", n // 2, chip_groups(n))
    other = lax.ppermute(mine, "tp", [(i, i ^ 1) for i in range(n)])
    even = lax.axis_index("tp") % 2 == 0
    both = jnp.stack([jnp.where(even, mine, other), jnp.where(even, other, mine)], axis=1)
    return both.reshape(n, *array.shape)


def shift(array, steps):
    n = lax.axis_size("fs")
    return lax.ppermute(array, "fs", [(i, (i + steps) % n) for i in range(n)])


def part_of(blocks, index, axis=0):
    return lax.dynamic_index_in_dim(blocks, index % blocks.shape[axis], axis, keepdims=False)


def scatter_sum(partial):
    n = lax.axis_size("fs")
    me = lax.axis_index("fs")
    far = n // (2 * NEAR)
    rows = partial.shape[0] // n
    width = partial.shape[1]
    f32 = jnp.float32

    blocks = partial.astype(BF16).reshape(far * 2, NEAR, rows, width)
    keep, ahead, across, behind = (part_of(blocks, me + d, 1) for d in range(NEAR))
    h = far
    ahead, behind = shift(ahead, 1), shift(behind, -1)
    low, high = shift(across[:h], 2), shift(across[h:], -2)
    total = keep.astype(f32) + ahead.astype(f32) + behind.astype(f32)
    total = total + jnp.concatenate([low, high], axis=0).astype(f32)

    blocks = total.astype(BF16).reshape(far, 2, rows, width)
    side = me // NEAR
    keep, other = part_of(blocks, side, 1), part_of(blocks, side + 1, 1)
    h = far // 2
    low, high = shift(other[:h], NEAR), shift(other[h:], -NEAR)
    total = keep.astype(f32) + jnp.concatenate([low, high], axis=0).astype(f32)

    got = exchange(total.astype(BF16), "fs", far_groups(n))
    return jnp.sum(got.astype(f32), axis=0)


def gather_tokens(own):
    n = lax.axis_size("fs")
    me = lax.axis_index("fs")
    far = n // (2 * NEAR)
    rows, width = own.shape

    got = spread_copies(own, "fs", far, far_groups(n))
    h = far // 2
    low, high = shift(got[:h], NEAR), shift(got[h:], -NEAR)
    side = me // NEAR
    both = jnp.zeros((far, 2, rows, width), own.dtype)
    for piece, index in ((got, side), (jnp.concatenate([low, high], axis=0), side + 1)):
        both = lax.dynamic_update_index_in_dim(both, piece, index % 2, 1)

    got = both.reshape(far * 2, rows, width)
    ahead, behind = shift(got, -1), shift(got, 1)
    low, high = shift(got[:far], 2), shift(got[far:], -2)
    out = jnp.zeros((far * 2, NEAR, rows, width), own.dtype)
    pieces = (got, ahead, jnp.concatenate([low, high], axis=0), behind)
    for d, piece in enumerate(pieces):
        out = lax.dynamic_update_index_in_dim(out, piece, (me + d) % NEAR, 1)
    return out.reshape(n * rows, width)


def on_device(
    prompt,
    gain_first,
    gate_first,
    up_first,
    down_first,
    gain_second,
    gate_second,
    up_second,
    down_second,
):
    n_fs = lax.axis_size("fs")
    n_tp = lax.axis_size("tp")
    rows, cols = gate_first.shape
    hid, dcols = down_first.shape
    width = prompt.shape[1]
    half = cols // dcols

    g1, u1 = fold(gain_first, gate_first), fold(gain_first, up_first)
    g2, u2 = fold(gain_second, gate_second), fold(gain_second, up_second)
    d1, d2 = down_first.astype(BF16), down_second.astype(BF16)

    pack = [m[:, k * dcols : (k + 1) * dcols] for m in (g2, u2) for k in range(half)] + [d2]
    whole = lax.all_gather(row_major(jnp.concatenate(pack, axis=0)), "fs", axis=0, tiled=True)
    whole = row_major(whole).reshape(n_fs, 2 * half * rows + hid, dcols)

    r = rows // n_tp
    lanes = cols * n_tp // n_fs
    per = n_fs // n_tp
    mats = jnp.stack([g1, u1, g2, u2]).reshape(4, n_tp, r, cols).transpose(1, 0, 2, 3)
    mats = exchange(mats, "tp")
    mats = mats.reshape(n_tp, 4, r, per, lanes).transpose(0, 3, 1, 2, 4).reshape(n_fs, 4, r, lanes)
    mats = exchange(mats, "fs")

    def packed(pair, down):
        parts = [down[:, k * lanes : (k + 1) * lanes] for k in range(dcols // lanes)]
        return jnp.concatenate([pair.reshape(-1, lanes), *parts], axis=0)

    def served_of(got):
        pair = got[:, : 2 * n_fs * r].reshape(n_tp, n_fs, 2, r, lanes)
        pair = pair.transpose(2, 1, 0, 3, 4).reshape(2, width, lanes)
        down = got[:, 2 * n_fs * r :].reshape(n_tp, dcols // lanes, hid, lanes)
        down = down.transpose(2, 0, 1, 3).reshape(hid, width)
        return pair[0], pair[1], down

    first = served_of(gather_tp(packed(mats[:, :2], d1)))
    second = served_of(lax.all_gather(packed(mats[:, 2:], d2), "tp", axis=0, tiled=False))

    stream = prompt.astype(jnp.float32)
    normed = normed_of(stream)
    gate = jnp.dot(normed, first[0], preferred_element_type=jnp.float32)
    up = jnp.dot(normed, first[1], preferred_element_type=jnp.float32)
    hidden = (jax.nn.silu(gate) * up).astype(BF16)
    partial = jnp.dot(hidden, first[2], preferred_element_type=jnp.float32)
    tokens = prompt.shape[0] // n_fs
    own = lax.dynamic_slice_in_dim(prompt, lax.axis_index("fs") * tokens, tokens, 0).astype(jnp.float32)
    own = own + 0.5 * scatter_sum(partial)

    normed = spread_copies(normed_of(own), "tp", n_tp).reshape(n_tp * tokens, width)
    normed, whole = lax.optimization_barrier((normed, whole))

    def columns(m):
        parts = [whole[:, (m * half + k) * rows : (m * half + k + 1) * rows].reshape(width, dcols) for k in range(half)]
        return jnp.concatenate([jnp.dot(normed, w, preferred_element_type=jnp.float32) for w in parts], axis=1)

    hidden = (jax.nn.silu(columns(0)) * columns(1)).astype(BF16)
    hidden = spread_copies(hidden, "tp", n_tp)
    hidden = hidden.transpose(1, 0, 2).reshape(n_tp * tokens, n_tp * cols)
    down = whole[:, 2 * half * rows :].reshape(n_fs * hid, dcols)
    out = jnp.dot(hidden, down, preferred_element_type=jnp.float32)
    out = exchange(out.reshape(n_tp, tokens, dcols), "tp")
    own = own + 0.5 * out.transpose(1, 0, 2).reshape(tokens, width)
    result = gather_tokens(own.astype(BF16))
    return (result, first[0], first[1], first[2], second[0], second[1], second[2])


def solution(mesh):
    return jax.shard_map(
        on_device,
        mesh=mesh,
        in_specs=(
            P(("grp", "tp"), None),
            P("fs"),
            P("fs", "tp"),
            P("fs", "tp"),
            P("fs", "tp"),
            P("fs"),
            P("fs", "tp"),
            P("fs", "tp"),
            P("fs", "tp"),
        ),
        out_specs=(
            P(("grp", "tp"), None),
            P("grp", "fs"),
            P("grp", "fs"),
            P("fs", "grp"),
            P("grp", "fs"),
            P("grp", "fs"),
            P("fs", "grp"),
        ),
        check_vma=False,
    )
```

```python
import jax
import jax.numpy as jnp
from jax import lax
from jax.experimental.layout import Layout, with_layout_constraint
from jax.sharding import PartitionSpec as P

EPS = 1e-06
NEAR = 4
BF16 = jnp.bfloat16


def fold(gain, weight):
    return (gain[:, None] * weight).astype(BF16)


def normed_of(stream):
    return (stream * lax.rsqrt(jnp.mean(stream * stream, axis=-1, keepdims=True) + EPS)).astype(BF16)


def row_major(array):
    return with_layout_constraint(array, Layout(major_to_minor=tuple(range(array.ndim))))


def exchange(blocks, axis, groups=None):
    return lax.all_to_all(blocks, axis, split_axis=0, concat_axis=0, tiled=True, axis_index_groups=groups)


def spread_copies(array, axis, members, groups=None):
    copies = jnp.broadcast_to(array, (members, *array.shape))
    if groups is not None and len(groups[0]) > members:
        copies = copies.reshape(len(groups[0]), *array.shape[1:])
    return exchange(copies, axis, groups)


def far_groups(n):
    return [list(range(i, n, NEAR)) for i in range(NEAR)]


def chip_groups(n):
    return [list(range(c, n, 2)) for c in range(2)]


def gather_tp(array):
    n = lax.axis_size("tp")
    mine = spread_copies(array, "tp", n // 2, chip_groups(n))
    other = lax.ppermute(mine, "tp", [(i, i ^ 1) for i in range(n)])
    even = lax.axis_index("tp") % 2 == 0
    both = jnp.stack([jnp.where(even, mine, other), jnp.where(even, other, mine)], axis=1)
    return both.reshape(n, *array.shape)


def shift(array, steps):
    n = lax.axis_size("fs")
    return lax.ppermute(array, "fs", [(i, (i + steps) % n) for i in range(n)])


def part_of(blocks, index, axis=0):
    return lax.dynamic_index_in_dim(blocks, index % blocks.shape[axis], axis, keepdims=False)


def scatter_sum(partial):
    n = lax.axis_size("fs")
    me = lax.axis_index("fs")
    far = n // NEAR
    rows = partial.shape[0] // n
    width = partial.shape[1]
    f32 = jnp.float32

    blocks = partial.astype(BF16).reshape(far, NEAR, rows, width)
    keep, ahead, across, behind = (part_of(blocks, me + d, 1) for d in range(NEAR))
    h = far // 2
    ahead, behind = shift(ahead, 1), shift(behind, -1)
    low, high = shift(across[:h], 2), shift(across[h:], -2)
    total = keep.astype(f32) + ahead.astype(f32) + behind.astype(f32)
    total = total + jnp.concatenate([low, high], axis=0).astype(f32)

    got = exchange(total.astype(BF16), "fs", far_groups(n))
    return jnp.sum(got.astype(f32), axis=0)


def gather_tokens(columns):
    n, n_tp = lax.axis_size("fs"), lax.axis_size("tp")
    me = lax.axis_index("fs")
    far = n // NEAR
    _, rows, cols = columns.shape
    groups = [[f * n_tp + t for f in g for t in range(n_tp)] for g in far_groups(n)]

    got = spread_copies(columns, ("fs", "tp"), far, groups)
    got = got.reshape(far, n_tp, rows, cols).transpose(0, 2, 1, 3).reshape(far, rows, n_tp * cols)
    h = far // 2
    ahead, behind = shift(got, -1), shift(got, 1)
    low, high = shift(got[:h], 2), shift(got[h:], -2)
    out = jnp.zeros((far, NEAR, rows, n_tp * cols), got.dtype)
    pieces = (got, ahead, jnp.concatenate([low, high], axis=0), behind)
    for d, piece in enumerate(pieces):
        out = lax.dynamic_update_index_in_dim(out, piece, (me + d) % NEAR, 1)
    return out.reshape(n * rows, n_tp * cols)


def on_device(
    prompt,
    gain_first,
    gate_first,
    up_first,
    down_first,
    gain_second,
    gate_second,
    up_second,
    down_second,
):
    n_fs = lax.axis_size("fs")
    n_tp = lax.axis_size("tp")
    rows, cols = gate_first.shape
    hid, dcols = down_first.shape
    width = prompt.shape[1]
    half = cols // dcols

    g1, u1 = fold(gain_first, gate_first), fold(gain_first, up_first)
    g2, u2 = fold(gain_second, gate_second), fold(gain_second, up_second)
    d1, d2 = down_first.astype(BF16), down_second.astype(BF16)

    pack = [m[:, k * dcols : (k + 1) * dcols] for m in (g2, u2) for k in range(half)] + [d2]
    whole = lax.all_gather(row_major(jnp.concatenate(pack, axis=0)), "fs", axis=0, tiled=True)
    whole = row_major(whole).reshape(n_fs, 2 * half * rows + hid, dcols)

    r = rows // n_tp
    lanes = cols * n_tp // n_fs
    per = n_fs // n_tp
    mats = jnp.stack([g1, u1, g2, u2]).reshape(4, n_tp, r, cols).transpose(1, 0, 2, 3)
    mats = exchange(mats, "tp")
    mats = mats.reshape(n_tp, 4, r, per, lanes).transpose(0, 3, 1, 2, 4).reshape(n_fs, 4, r, lanes)
    mats = exchange(mats, "fs")

    def packed(pair, down):
        parts = [down[:, k * lanes : (k + 1) * lanes] for k in range(dcols // lanes)]
        return jnp.concatenate([pair.reshape(-1, lanes), *parts], axis=0)

    def served_of(got):
        cut = 2 * n_fs * r
        pair = got[:, :cut].reshape(n_tp, n_fs, 2, r, lanes)
        pair = pair.transpose(2, 1, 0, 3, 4).reshape(2, width, lanes)
        down = got[:, cut:].reshape(n_tp, dcols // lanes, hid, lanes)
        return pair[0], pair[1], down.transpose(2, 0, 1, 3).reshape(hid, width)

    first = served_of(gather_tp(packed(mats[:, :2], d1)))
    second = served_of(lax.all_gather(packed(mats[:, 2:], d2), "tp", axis=0, tiled=False))

    stream = prompt.astype(jnp.float32)
    normed = normed_of(stream)
    gate = jnp.dot(normed, first[0], preferred_element_type=jnp.float32)
    up = jnp.dot(normed, first[1], preferred_element_type=jnp.float32)
    hidden = (jax.nn.silu(gate) * up).astype(BF16)
    partial = jnp.dot(hidden, first[2], preferred_element_type=jnp.float32)
    tokens = prompt.shape[0] // n_fs
    own = lax.dynamic_slice_in_dim(prompt, lax.axis_index("fs") * tokens, tokens, 0).astype(jnp.float32)
    own = own + 0.5 * scatter_sum(partial)

    high = own.astype(BF16)
    low = (own - high.astype(jnp.float32)).astype(BF16)
    halves = [h.reshape(tokens, n_tp, dcols).transpose(1, 0, 2) for h in (high, low)]
    copies = jnp.broadcast_to(normed_of(own), (n_tp, tokens, width))
    got = exchange(jnp.concatenate([copies, *halves], axis=2), "tp")
    normed = got[:, :, :width].reshape(n_tp * tokens, width)
    base = got[:, :, width : width + dcols].astype(jnp.float32) + got[:, :, width + dcols :].astype(jnp.float32)
    normed, whole = lax.optimization_barrier((normed, whole))

    def columns(m):
        parts = [whole[:, (m * half + k) * rows : (m * half + k + 1) * rows].reshape(width, dcols) for k in range(half)]
        return jnp.concatenate([jnp.dot(normed, w, preferred_element_type=jnp.float32) for w in parts], axis=1)

    hidden = (jax.nn.silu(columns(0)) * columns(1)).astype(BF16)
    hidden = spread_copies(hidden, "tp", n_tp)
    hidden = hidden.transpose(1, 0, 2).reshape(n_tp * tokens, n_tp * cols)
    down = whole[:, 2 * half * rows :].reshape(n_fs * hid, dcols)
    out = jnp.dot(hidden, down, preferred_element_type=jnp.float32)
    result = gather_tokens((base + 0.5 * out.reshape(n_tp, tokens, dcols)).astype(BF16))
    return (result, first[0], first[1], first[2], second[0], second[1], second[2])


def solution(mesh):
    return jax.shard_map(
        on_device,
        mesh=mesh,
        in_specs=(
            P(("grp", "tp"), None),
            P("fs"),
            P("fs", "tp"),
            P("fs", "tp"),
            P("fs", "tp"),
            P("fs"),
            P("fs", "tp"),
            P("fs", "tp"),
            P("fs", "tp"),
        ),
        out_specs=(
            P(("grp", "tp"), None),
            P("grp", "fs"),
            P("grp", "fs"),
            P("fs", "grp"),
            P("grp", "fs"),
            P("grp", "fs"),
            P("fs", "grp"),
        ),
        check_vma=False,
    )
```

```python
import jax
import jax.numpy as jnp
from jax import lax
from jax.experimental import pallas as pl
from jax.experimental.layout import Layout, with_layout_constraint
from jax.experimental.pallas import tpu as pltpu
from jax.sharding import PartitionSpec as P

EPS = 1e-06
NEAR = 4
BF16 = jnp.bfloat16


def fold(gain, weight):
    return (gain[:, None] * weight).astype(BF16)


def normed_of(stream):
    return (stream * lax.rsqrt(jnp.mean(stream * stream, axis=-1, keepdims=True) + EPS)).astype(BF16)


def row_major(array):
    return with_layout_constraint(array, Layout(major_to_minor=tuple(range(array.ndim))))


def exchange(blocks, axis, groups=None):
    return lax.all_to_all(blocks, axis, split_axis=0, concat_axis=0, tiled=True, axis_index_groups=groups)


def spread_copies(array, axis, members, groups=None):
    copies = jnp.broadcast_to(array, (members, *array.shape))
    if groups is not None and len(groups[0]) > members:
        copies = copies.reshape(len(groups[0]), *array.shape[1:])
    return exchange(copies, axis, groups)


def far_groups(n):
    return [list(range(i, n, NEAR)) for i in range(NEAR)]


def chip_groups(n):
    return [list(range(c, n, 2)) for c in range(2)]


def gather_tp(array):
    n = lax.axis_size("tp")
    mine = spread_copies(array, "tp", n // 2, chip_groups(n))
    other = lax.ppermute(mine, "tp", [(i, i ^ 1) for i in range(n)])
    even = lax.axis_index("tp") % 2 == 0
    both = jnp.stack([jnp.where(even, mine, other), jnp.where(even, other, mine)], axis=1)
    return both.reshape(n, *array.shape)


def shift_tp(array, steps):
    n = lax.axis_size("tp")
    return lax.ppermute(array, "tp", [(i, (i + steps) % n) for i in range(n)])


def gather_tp_beside(array):
    n = lax.axis_size("tp")
    chips = n // 2
    me = lax.axis_index("tp")
    mine = jnp.zeros((chips, *array.shape), array.dtype)
    for d in range(chips):
        piece = array if d == 0 else shift_tp(array, -2 * d)
        mine = lax.dynamic_update_index_in_dim(mine, piece, (me // 2 + d) % chips, 0)
    other = lax.ppermute(mine, "tp", [(i, i ^ 1) for i in range(n)])
    even = me % 2 == 0
    both = jnp.stack([jnp.where(even, mine, other), jnp.where(even, other, mine)], axis=1)
    return both.reshape(n, *array.shape)


def shift(array, steps):
    n = lax.axis_size("fs")
    return lax.ppermute(array, "fs", [(i, (i + steps) % n) for i in range(n)])


def part_of(blocks, index, axis=0):
    return lax.dynamic_index_in_dim(blocks, index % blocks.shape[axis], axis, keepdims=False)


def scatter_sum(partial):
    n = lax.axis_size("fs")
    me = lax.axis_index("fs")
    far = n // NEAR
    rows = partial.shape[0] // n
    width = partial.shape[1]
    f32 = jnp.float32

    blocks = partial.astype(BF16).reshape(far, NEAR, rows, width)
    keep, ahead, across, behind = (part_of(blocks, me + d, 1) for d in range(NEAR))
    h = far // 2
    ahead, behind = shift(ahead, 1), shift(behind, -1)
    low, high = shift(across[:h], 2), shift(across[h:], -2)
    total = keep.astype(f32) + ahead.astype(f32) + behind.astype(f32)
    total = total + jnp.concatenate([low, high], axis=0).astype(f32)

    got = exchange(total.astype(BF16), "fs", far_groups(n))
    return jnp.sum(got.astype(f32), axis=0)


def gather_tokens(own):
    n = lax.axis_size("fs")
    me = lax.axis_index("fs")
    far = n // NEAR
    rows, width = own.shape

    got = spread_copies(own, "fs", far, far_groups(n))
    h = far // 2
    ahead, behind = shift(got, -1), shift(got, 1)
    low, high = shift(got[:h], 2), shift(got[h:], -2)
    out = jnp.zeros((far, NEAR, rows, width), own.dtype)
    pieces = (got, ahead, jnp.concatenate([low, high], axis=0), behind)
    for d, piece in enumerate(pieces):
        out = lax.dynamic_update_index_in_dim(out, piece, (me + d) % NEAR, 1)
    return out.reshape(n * rows, width)


STEPS = 4


def hidden_kernel(normed, whole):
    tokens, width = normed.shape
    planes, _, cols = whole.shape
    rows = width // planes
    halves = 2
    per = planes // STEPS
    group = 256 // rows

    def body(x_ref, w_ref, o_ref, acc_ref):
        step = pl.program_id(0)

        @pl.when(step == 0)
        def _():
            acc_ref[...] = jnp.zeros_like(acc_ref)

        for j in range(per // group):
            x = x_ref[:, j * group * rows : (j + 1) * group * rows]
            for m in range(2 * halves):
                w = jnp.concatenate(
                    [w_ref[j * group + k, m * rows : (m + 1) * rows, :] for k in range(group)], axis=0
                )
                acc_ref[m] += jnp.dot(x, w, preferred_element_type=jnp.float32)

        @pl.when(step == STEPS - 1)
        def _():
            for m in range(halves):
                gate, up = acc_ref[m], acc_ref[halves + m]
                o_ref[:, m * cols : (m + 1) * cols] = (gate / (1.0 + jnp.exp(-gate)) * up).astype(BF16)

    return pl.pallas_call(
        body,
        grid=(STEPS,),
        in_specs=[
            pl.BlockSpec((tokens, width // STEPS), lambda i: (0, i)),
            pl.BlockSpec((per, 2 * halves * rows, cols), lambda i: (i, 0, 0)),
        ],
        out_specs=pl.BlockSpec((tokens, halves * cols), lambda i: (0, 0)),
        out_shape=jax.ShapeDtypeStruct((tokens, halves * cols), BF16),
        scratch_shapes=[pltpu.VMEM((2 * halves, tokens, cols), jnp.float32)],
        name="hidden_second",
    )(normed, whole)


def down_kernel(hidden, whole, hid):
    n_tp, tokens, cols = hidden.shape
    planes, rows, width = whole.shape
    per = planes // STEPS
    blocks = n_tp // STEPS
    each = per // blocks

    def body(h_ref, w_ref, o_ref):
        step = pl.program_id(0)

        @pl.when(step == 0)
        def _():
            o_ref[...] = jnp.zeros_like(o_ref)

        for b in range(blocks):
            w = w_ref[b * each : (b + 1) * each].reshape(cols, width)
            o_ref[...] += jnp.dot(h_ref[b], w, preferred_element_type=jnp.float32)

    return pl.pallas_call(
        body,
        grid=(STEPS,),
        in_specs=[
            pl.BlockSpec((blocks, tokens, cols), lambda i: (i, 0, 0)),
            pl.BlockSpec((per, hid, width), lambda i: (i, rows // hid - 1, 0)),
        ],
        out_specs=pl.BlockSpec((tokens, width), lambda i: (0, 0)),
        out_shape=jax.ShapeDtypeStruct((tokens, width), jnp.float32),
        name="down_second",
    )(hidden, whole)


def on_device(
    prompt,
    gain_first,
    gate_first,
    up_first,
    down_first,
    gain_second,
    gate_second,
    up_second,
    down_second,
):
    n_fs = lax.axis_size("fs")
    n_tp = lax.axis_size("tp")
    rows, cols = gate_first.shape
    hid, dcols = down_first.shape
    width = prompt.shape[1]
    half = cols // dcols

    g1, u1 = fold(gain_first, gate_first), fold(gain_first, up_first)
    g2, u2 = fold(gain_second, gate_second), fold(gain_second, up_second)
    d1, d2 = down_first.astype(BF16), down_second.astype(BF16)

    pack = [m[:, k * dcols : (k + 1) * dcols] for m in (g2, u2) for k in range(half)] + [d2]
    whole = lax.all_gather(row_major(jnp.concatenate(pack, axis=0)), "fs", axis=0, tiled=True)
    whole = row_major(whole).reshape(n_fs, 2 * half * rows + hid, dcols)

    r = rows // n_tp
    lanes = cols * n_tp // n_fs
    per = n_fs // n_tp
    mats = jnp.stack([g1, u1, g2, u2]).reshape(4, n_tp, r, cols).transpose(1, 0, 2, 3)
    mats = exchange(mats, "tp")
    mats = mats.reshape(n_tp, 4, r, per, lanes).transpose(0, 3, 1, 2, 4).reshape(n_fs, 4, r, lanes)
    mats, d1 = lax.optimization_barrier((mats, d1))
    mats = exchange(mats, "fs")

    def in_lanes(down):
        return jnp.concatenate([down[:, k * lanes : (k + 1) * lanes] for k in range(dcols // lanes)], axis=0)

    def pair_of(got):
        pair = got.reshape(n_tp, n_fs, 2, r, lanes).transpose(2, 1, 0, 3, 4).reshape(2, width, lanes)
        return pair[0], pair[1]

    def down_of(got):
        down = got.reshape(n_tp, dcols // lanes, hid, lanes)
        return down.transpose(2, 0, 1, 3).reshape(hid, width)

    mats, down = lax.optimization_barrier((mats, gather_tp_beside(in_lanes(d1))))
    first = (*pair_of(gather_tp(mats[:, :2].reshape(-1, lanes))), down_of(down))
    rest = jnp.concatenate([mats[:, 2:].reshape(-1, lanes), in_lanes(d2)], axis=0)
    rest = lax.all_gather(rest, "tp", axis=0, tiled=False)
    cut = 2 * n_fs * r
    second = (*pair_of(rest[:, :cut]), down_of(rest[:, cut:]))

    stream = prompt.astype(jnp.float32)
    normed = normed_of(stream)
    gate = jnp.dot(normed, first[0], preferred_element_type=jnp.float32)
    up = jnp.dot(normed, first[1], preferred_element_type=jnp.float32)
    hidden = (jax.nn.silu(gate) * up).astype(BF16)
    partial = jnp.dot(hidden, first[2], preferred_element_type=jnp.float32)
    tokens = prompt.shape[0] // n_fs
    own = lax.dynamic_slice_in_dim(prompt, lax.axis_index("fs") * tokens, tokens, 0).astype(jnp.float32)
    own = own + 0.5 * scatter_sum(partial)

    normed = spread_copies(normed_of(own), "tp", n_tp).reshape(n_tp * tokens, width)
    hidden = spread_copies(hidden_kernel(normed, whole), "tp", n_tp)
    out = down_kernel(hidden, whole, hid)
    out = exchange(out.reshape(n_tp, tokens, dcols), "tp")
    own = own + 0.5 * out.transpose(1, 0, 2).reshape(tokens, width)
    result = gather_tokens(own.astype(BF16))
    return (result, first[0], first[1], first[2], second[0], second[1], second[2])


def solution(mesh):
    return jax.shard_map(
        on_device,
        mesh=mesh,
        in_specs=(
            P(("grp", "tp"), None),
            P("fs"),
            P("fs", "tp"),
            P("fs", "tp"),
            P("fs", "tp"),
            P("fs"),
            P("fs", "tp"),
            P("fs", "tp"),
            P("fs", "tp"),
        ),
        out_specs=(
            P(("grp", "tp"), None),
            P("grp", "fs"),
            P("grp", "fs"),
            P("fs", "grp"),
            P("grp", "fs"),
            P("grp", "fs"),
            P("fs", "grp"),
        ),
        check_vma=False,
    )
```

```python
import jax
import jax.numpy as jnp
from jax import lax
from jax.experimental import pallas as pl
from jax.experimental.layout import Layout, with_layout_constraint
from jax.experimental.pallas import tpu as pltpu
from jax.sharding import PartitionSpec as P

EPS = 1e-06
NEAR = 4
BF16 = jnp.bfloat16


def fold(gain, weight):
    return (gain[:, None] * weight).astype(BF16)


def normed_of(stream):
    return (stream * lax.rsqrt(jnp.mean(stream * stream, axis=-1, keepdims=True) + EPS)).astype(BF16)


def row_major(array):
    return with_layout_constraint(array, Layout(major_to_minor=tuple(range(array.ndim))))


def exchange(blocks, axis, groups=None):
    return lax.all_to_all(blocks, axis, split_axis=0, concat_axis=0, tiled=True, axis_index_groups=groups)


def spread_copies(array, axis, members, groups=None):
    copies = jnp.broadcast_to(array, (members, *array.shape))
    if groups is not None and len(groups[0]) > members:
        copies = copies.reshape(len(groups[0]), *array.shape[1:])
    return exchange(copies, axis, groups)


def far_groups(n):
    return [list(range(i, n, NEAR)) for i in range(NEAR)]


def chip_groups(n):
    return [list(range(c, n, 2)) for c in range(2)]


def gather_tp(array):
    n = lax.axis_size("tp")
    mine = spread_copies(array, "tp", n // 2, chip_groups(n))
    other = lax.ppermute(mine, "tp", [(i, i ^ 1) for i in range(n)])
    even = lax.axis_index("tp") % 2 == 0
    both = jnp.stack([jnp.where(even, mine, other), jnp.where(even, other, mine)], axis=1)
    return both.reshape(n, *array.shape)


def shift_tp(array, steps):
    n = lax.axis_size("tp")
    return lax.ppermute(array, "tp", [(i, (i + steps) % n) for i in range(n)])


def gather_tp_beside(array):
    n = lax.axis_size("tp")
    chips = n // 2
    me = lax.axis_index("tp")
    mine = jnp.zeros((chips, *array.shape), array.dtype)
    for d in range(chips):
        piece = array if d == 0 else shift_tp(array, -2 * d)
        mine = lax.dynamic_update_index_in_dim(mine, piece, (me // 2 + d) % chips, 0)
    other = lax.ppermute(mine, "tp", [(i, i ^ 1) for i in range(n)])
    even = me % 2 == 0
    both = jnp.stack([jnp.where(even, mine, other), jnp.where(even, other, mine)], axis=1)
    return both.reshape(n, *array.shape)


def shift(array, steps):
    n = lax.axis_size("fs")
    return lax.ppermute(array, "fs", [(i, (i + steps) % n) for i in range(n)])


def part_of(blocks, index, axis=0):
    return lax.dynamic_index_in_dim(blocks, index % blocks.shape[axis], axis, keepdims=False)


def scatter_sum(partial):
    n = lax.axis_size("fs")
    me = lax.axis_index("fs")
    far = n // NEAR
    rows = partial.shape[0] // n
    width = partial.shape[1]
    f32 = jnp.float32

    blocks = partial.astype(BF16).reshape(far, NEAR, rows, width)
    keep, ahead, across, behind = (part_of(blocks, me + d, 1) for d in range(NEAR))
    h = far // 2
    ahead, behind = shift(ahead, 1), shift(behind, -1)
    low, high = shift(across[:h], 2), shift(across[h:], -2)
    total = keep.astype(f32) + ahead.astype(f32) + behind.astype(f32)
    total = total + jnp.concatenate([low, high], axis=0).astype(f32)

    got = exchange(total.astype(BF16), "fs", far_groups(n))
    return jnp.sum(got.astype(f32), axis=0)


def gather_tokens(own):
    n = lax.axis_size("fs")
    me = lax.axis_index("fs")
    far = n // NEAR
    rows, width = own.shape

    got = spread_copies(own, "fs", far, far_groups(n))
    h = far // 2
    ahead, behind = shift(got, -1), shift(got, 1)
    low, high = shift(got[:h], 2), shift(got[h:], -2)
    out = jnp.zeros((far, NEAR, rows, width), own.dtype)
    pieces = (got, ahead, jnp.concatenate([low, high], axis=0), behind)
    for d, piece in enumerate(pieces):
        out = lax.dynamic_update_index_in_dim(out, piece, (me + d) % NEAR, 1)
    return out.reshape(n * rows, width)


STEPS = 4
PAIR = 2


def pair_groups(n, n_tp):
    return [[(f + b) * n_tp + t for b in (0, PAIR) for t in range(n_tp)] for f in range(n) if not f & PAIR]


def role_groups(n):
    return [[f for f in range(n) if f & PAIR == p] for p in (0, PAIR)]


def hidden_kernel(normed, whole):
    tokens, width = normed.shape
    planes, _, cols = whole.shape
    rows = width // (2 * planes)
    per = planes // STEPS

    def body(x_ref, w_ref, o_ref, acc_ref):
        step = pl.program_id(0)

        @pl.when(step == 0)
        def _():
            acc_ref[...] = jnp.zeros_like(acc_ref)

        for k in range(per // 2):
            x = x_ref[:, 4 * k * rows : 4 * (k + 1) * rows]
            for m in range(2):
                pieces = [
                    w_ref[2 * k + e, (2 * m + h) * rows : (2 * m + h + 1) * rows, :] for h in range(2) for e in range(2)
                ]
                w = jnp.concatenate(pieces, axis=0)
                acc_ref[m] += jnp.dot(x, w, preferred_element_type=jnp.float32)

        @pl.when(step == STEPS - 1)
        def _():
            gate, up = acc_ref[0], acc_ref[1]
            o_ref[...] = (gate / (1.0 + jnp.exp(-gate)) * up).astype(BF16)

    return pl.pallas_call(
        body,
        grid=(STEPS,),
        in_specs=[
            pl.BlockSpec((tokens, width // STEPS), lambda i: (0, i)),
            pl.BlockSpec((per, 4 * rows, cols), lambda i: (i, 0, 0)),
        ],
        out_specs=pl.BlockSpec((tokens, cols), lambda i: (0, 0)),
        out_shape=jax.ShapeDtypeStruct((tokens, cols), BF16),
        scratch_shapes=[pltpu.VMEM((2, tokens, cols), jnp.float32)],
        name="hidden_second",
    )(normed, whole)


def down_kernel(hidden, whole, hid):
    n_tp, tokens, cols = hidden.shape
    planes, rows, width = whole.shape
    per = planes // STEPS
    blocks = n_tp // STEPS
    each = per // blocks

    def body(h_ref, w_ref, o_ref):
        step = pl.program_id(0)

        @pl.when(step == 0)
        def _():
            o_ref[...] = jnp.zeros_like(o_ref)

        for b in range(blocks):
            w = w_ref[b * each : (b + 1) * each].reshape(cols, width)
            o_ref[...] += jnp.dot(h_ref[b], w, preferred_element_type=jnp.float32)

    return pl.pallas_call(
        body,
        grid=(STEPS,),
        in_specs=[
            pl.BlockSpec((blocks, tokens, cols), lambda i: (i, 0, 0)),
            pl.BlockSpec((per, hid, width), lambda i: (i, rows // hid - 1, 0)),
        ],
        out_specs=pl.BlockSpec((tokens, width), lambda i: (0, 0)),
        out_shape=jax.ShapeDtypeStruct((tokens, width), jnp.float32),
        name="down_second",
    )(hidden, whole)


def on_device(
    prompt,
    gain_first,
    gate_first,
    up_first,
    down_first,
    gain_second,
    gate_second,
    up_second,
    down_second,
):
    n_fs = lax.axis_size("fs")
    n_tp = lax.axis_size("tp")
    rows, cols = gate_first.shape
    hid, dcols = down_first.shape
    width = prompt.shape[1]

    g1, u1 = fold(gain_first, gate_first), fold(gain_first, up_first)
    g2, u2 = fold(gain_second, gate_second), fold(gain_second, up_second)
    d1, d2 = down_first.astype(BF16), down_second.astype(BF16)

    me = lax.axis_index("fs")
    upper = me & PAIR == PAIR
    low = jnp.concatenate([g2[:, : cols // 2], u2[:, : cols // 2]], axis=0)
    high = jnp.concatenate([g2[:, cols // 2 :], u2[:, cols // 2 :]], axis=0)
    mine = jnp.where(upper, high, low)
    theirs = lax.ppermute(jnp.where(upper, low, high), "fs", [(f, f ^ PAIR) for f in range(n_fs)])

    r = rows // n_tp
    lanes = cols * n_tp // n_fs
    per = n_fs // n_tp
    mats = jnp.stack([g1, u1, g2, u2]).reshape(4, n_tp, r, cols).transpose(1, 0, 2, 3)
    mats = exchange(mats, "tp")
    mats, theirs = lax.optimization_barrier((mats, theirs))
    above, below = jnp.where(upper, mine, theirs), jnp.where(upper, theirs, mine)
    pack = [below[:rows], above[:rows], below[rows:], above[rows:], d2]
    whole = lax.all_gather(
        row_major(jnp.concatenate(pack, axis=0)), "fs", axis=0, tiled=True, axis_index_groups=role_groups(n_fs)
    )
    whole = row_major(whole).reshape(n_fs // 2, 4 * rows + hid, cols // 2)
    mats = mats.reshape(n_tp, 4, r, per, lanes).transpose(0, 3, 1, 2, 4).reshape(n_fs, 4, r, lanes)
    mats, d1 = lax.optimization_barrier((mats, d1))
    mats = exchange(mats, "fs")

    def in_lanes(down):
        return jnp.concatenate([down[:, k * lanes : (k + 1) * lanes] for k in range(dcols // lanes)], axis=0)

    def pair_of(got):
        pair = got.reshape(n_tp, n_fs, 2, r, lanes).transpose(2, 1, 0, 3, 4).reshape(2, width, lanes)
        return pair[0], pair[1]

    def down_of(got):
        down = got.reshape(n_tp, dcols // lanes, hid, lanes)
        return down.transpose(2, 0, 1, 3).reshape(hid, width)

    mats, down = lax.optimization_barrier((mats, gather_tp_beside(in_lanes(d1))))
    first = (*pair_of(gather_tp(mats[:, :2].reshape(-1, lanes))), down_of(down))
    rest = jnp.concatenate([mats[:, 2:].reshape(-1, lanes), in_lanes(d2)], axis=0)
    rest = lax.all_gather(rest, "tp", axis=0, tiled=False)
    cut = 2 * n_fs * r
    second = (*pair_of(rest[:, :cut]), down_of(rest[:, cut:]))

    stream = prompt.astype(jnp.float32)
    normed = normed_of(stream)
    gate = jnp.dot(normed, first[0], preferred_element_type=jnp.float32)
    up = jnp.dot(normed, first[1], preferred_element_type=jnp.float32)
    hidden = (jax.nn.silu(gate) * up).astype(BF16)
    partial = jnp.dot(hidden, first[2], preferred_element_type=jnp.float32)
    tokens = prompt.shape[0] // n_fs
    own = lax.dynamic_slice_in_dim(prompt, me * tokens, tokens, 0).astype(jnp.float32)
    own = own + 0.5 * scatter_sum(partial)

    both = pair_groups(n_fs, n_tp)
    members = 2 * n_tp
    normed = spread_copies(normed_of(own), ("fs", "tp"), members, both).reshape(members * tokens, width)
    hidden = spread_copies(hidden_kernel(normed, whole), "tp", n_tp)
    out = down_kernel(hidden, whole, hid)
    out = exchange(out.reshape(members, tokens, dcols), ("fs", "tp"), both)
    out = jnp.sum(out.reshape(2, n_tp, tokens, dcols), axis=0)
    own = own + 0.5 * out.transpose(1, 0, 2).reshape(tokens, width)
    result = gather_tokens(own.astype(BF16))
    return (result, first[0], first[1], first[2], second[0], second[1], second[2])


def solution(mesh):
    return jax.shard_map(
        on_device,
        mesh=mesh,
        in_specs=(
            P(("grp", "tp"), None),
            P("fs"),
            P("fs", "tp"),
            P("fs", "tp"),
            P("fs", "tp"),
            P("fs"),
            P("fs", "tp"),
            P("fs", "tp"),
            P("fs", "tp"),
        ),
        out_specs=(
            P(("grp", "tp"), None),
            P("grp", "fs"),
            P("grp", "fs"),
            P("fs", "grp"),
            P("grp", "fs"),
            P("grp", "fs"),
            P("fs", "grp"),
        ),
        check_vma=False,
    )
```

```python
import jax
import jax.numpy as jnp
from jax import lax
from jax.experimental import pallas as pl
from jax.experimental.layout import Layout, with_layout_constraint
from jax.experimental.pallas import tpu as pltpu
from jax.sharding import PartitionSpec as P


EPS = 1e-06
NEAR = 4
BF16 = jnp.bfloat16


def fold(gain, weight):
    return (gain[:, None] * weight).astype(BF16)


def normed_of(stream):
    return (stream * lax.rsqrt(jnp.mean(stream * stream, axis=-1, keepdims=True) + EPS)).astype(BF16)


def row_major(array):
    return with_layout_constraint(array, Layout(major_to_minor=tuple(range(array.ndim))))


def exchange(blocks, axis, groups=None):
    return lax.all_to_all(blocks, axis, split_axis=0, concat_axis=0, tiled=True, axis_index_groups=groups)


def spread_copies(array, axis, members, groups=None):
    copies = jnp.broadcast_to(array, (members, *array.shape))
    if groups is not None and len(groups[0]) > members:
        copies = copies.reshape(len(groups[0]), *array.shape[1:])
    return exchange(copies, axis, groups)


def far_groups(n):
    return [list(range(i, n, NEAR)) for i in range(NEAR)]


def chip_groups(n):
    return [list(range(c, n, 2)) for c in range(2)]


def gather_tp(array):
    n = lax.axis_size("tp")
    mine = spread_copies(array, "tp", n // 2, chip_groups(n))
    other = lax.ppermute(mine, "tp", [(i, i ^ 1) for i in range(n)])
    even = lax.axis_index("tp") % 2 == 0
    both = jnp.stack([jnp.where(even, mine, other), jnp.where(even, other, mine)], axis=1)
    return both.reshape(n, *array.shape)


def shift_tp(array, steps):
    n = lax.axis_size("tp")
    return lax.ppermute(array, "tp", [(i, (i + steps) % n) for i in range(n)])


def gather_tp_beside(array):
    n = lax.axis_size("tp")
    chips = n // 2
    me = lax.axis_index("tp")
    mine = jnp.zeros((chips, *array.shape), array.dtype)
    for d in range(chips):
        piece = array if d == 0 else shift_tp(array, -2 * d)
        mine = lax.dynamic_update_index_in_dim(mine, piece, (me // 2 + d) % chips, 0)
    other = lax.ppermute(mine, "tp", [(i, i ^ 1) for i in range(n)])
    even = me % 2 == 0
    both = jnp.stack([jnp.where(even, mine, other), jnp.where(even, other, mine)], axis=1)
    return both.reshape(n, *array.shape)


def shift(array, steps):
    n = lax.axis_size("fs")
    return lax.ppermute(array, "fs", [(i, (i + steps) % n) for i in range(n)])


def part_of(blocks, index, axis=0):
    return lax.dynamic_index_in_dim(blocks, index % blocks.shape[axis], axis, keepdims=False)


def scatter_sum(partial, rest, packed):
    n = lax.axis_size("fs")
    me = lax.axis_index("fs")
    far = n // NEAR
    rows = partial.shape[0] // n
    width = partial.shape[1]
    f32 = jnp.float32

    blocks = partial.astype(BF16).reshape(far, NEAR, rows, width)
    keep, ahead, across, behind = (part_of(blocks, me + d, 1) for d in range(NEAR))
    h = far // 2
    ahead, behind = shift(ahead, 1), shift(behind, -1)
    low, high = shift(across[:h], 2), shift(across[h:], -2)
    total = keep.astype(f32) + ahead.astype(f32) + behind.astype(f32)
    total = total + jnp.concatenate([low, high], axis=0).astype(f32)

    total, rest = lax.optimization_barrier((total.astype(BF16), rest))
    got = exchange(total, "fs", far_groups(n))
    rest = packed(*rest)
    rest = gather_tp_beside(rest)
    got, rest = lax.optimization_barrier((got, rest))
    return jnp.sum(got.astype(f32), axis=0), rest


def gather_tokens(own):
    n = lax.axis_size("fs")
    me = lax.axis_index("fs")
    far = n // NEAR
    rows, width = own.shape

    got = spread_copies(own, "fs", far, far_groups(n))
    h = far // 2
    ahead, behind = shift(got, -1), shift(got, 1)
    low, high = shift(got[:h], 2), shift(got[h:], -2)
    out = jnp.zeros((far, NEAR, rows, width), own.dtype)
    pieces = (got, ahead, jnp.concatenate([low, high], axis=0), behind)
    for d, piece in enumerate(pieces):
        out = lax.dynamic_update_index_in_dim(out, piece, (me + d) % NEAR, 1)
    return out.reshape(n * rows, width)


STEPS = 4
PAIR = 2


def pair_groups(n, n_tp):
    return [[(f + b) * n_tp + t for b in (0, PAIR) for t in range(n_tp)] for f in range(n) if not f & PAIR]


def role_groups(n):
    return [[f for f in range(n) if f & PAIR == p] for p in (0, PAIR)]


def hidden_kernel(normed, whole):
    tokens, width = normed.shape
    planes, _, cols = whole.shape
    rows = width // (2 * planes)
    per = planes // STEPS

    def body(x_ref, w_ref, o_ref, acc_ref):
        step = pl.program_id(0)

        @pl.when(step == 0)
        def _():
            acc_ref[...] = jnp.zeros_like(acc_ref)

        for k in range(per // 2):
            x = x_ref[:, 4 * k * rows : 4 * (k + 1) * rows]
            for m in range(2):
                pieces = [
                    w_ref[2 * k + e, (2 * m + h) * rows : (2 * m + h + 1) * rows, :] for h in range(2) for e in range(2)
                ]
                w = jnp.concatenate(pieces, axis=0)
                acc_ref[m] += jnp.dot(x, w, preferred_element_type=jnp.float32)

        @pl.when(step == STEPS - 1)
        def _():
            gate, up = acc_ref[0], acc_ref[1]
            o_ref[...] = (gate / (1.0 + jnp.exp(-gate)) * up).astype(BF16)

    return pl.pallas_call(
        body,
        grid=(STEPS,),
        in_specs=[
            pl.BlockSpec((tokens, width // STEPS), lambda i: (0, i)),
            pl.BlockSpec((per, 4 * rows, cols), lambda i: (i, 0, 0)),
        ],
        out_specs=pl.BlockSpec((tokens, cols), lambda i: (0, 0)),
        out_shape=jax.ShapeDtypeStruct((tokens, cols), BF16),
        scratch_shapes=[pltpu.VMEM((2, tokens, cols), jnp.float32)],
        name="hidden_second",
    )(normed, whole)


def down_kernel(hidden, whole, hid):
    n_tp, tokens, cols = hidden.shape
    planes, rows, width = whole.shape
    per = planes // STEPS
    blocks = n_tp // STEPS
    each = per // blocks

    def body(h_ref, w_ref, o_ref):
        step = pl.program_id(0)

        @pl.when(step == 0)
        def _():
            o_ref[...] = jnp.zeros_like(o_ref)

        for b in range(blocks):
            w = w_ref[b * each : (b + 1) * each].reshape(cols, width)
            o_ref[...] += jnp.dot(h_ref[b], w, preferred_element_type=jnp.float32)

    return pl.pallas_call(
        body,
        grid=(STEPS,),
        in_specs=[
            pl.BlockSpec((blocks, tokens, cols), lambda i: (i, 0, 0)),
            pl.BlockSpec((per, hid, width), lambda i: (i, rows // hid - 1, 0)),
        ],
        out_specs=pl.BlockSpec((tokens, width), lambda i: (0, 0)),
        out_shape=jax.ShapeDtypeStruct((tokens, width), jnp.float32),
        name="down_second",
    )(hidden, whole)


def on_device(
    prompt,
    gain_first,
    gate_first,
    up_first,
    down_first,
    gain_second,
    gate_second,
    up_second,
    down_second,
):
    n_fs = lax.axis_size("fs")
    n_tp = lax.axis_size("tp")
    rows, cols = gate_first.shape
    hid, dcols = down_first.shape
    width = prompt.shape[1]

    g1, u1 = fold(gain_first, gate_first), fold(gain_first, up_first)
    g2, u2 = fold(gain_second, gate_second), fold(gain_second, up_second)
    d1, d2 = down_first.astype(BF16), down_second.astype(BF16)

    me = lax.axis_index("fs")
    upper = me & PAIR == PAIR
    low = jnp.concatenate([g2[:, : cols // 2], u2[:, : cols // 2]], axis=0)
    high = jnp.concatenate([g2[:, cols // 2 :], u2[:, cols // 2 :]], axis=0)
    mine = jnp.where(upper, high, low)
    theirs = lax.ppermute(jnp.where(upper, low, high), "fs", [(f, f ^ PAIR) for f in range(n_fs)])

    r = rows // n_tp
    lanes = cols * n_tp // n_fs
    per = n_fs // n_tp
    mats = jnp.stack([g1, u1, g2, u2]).reshape(4, n_tp, r, cols).transpose(1, 0, 2, 3)
    mats = exchange(mats, "tp")
    mats, theirs = lax.optimization_barrier((mats, theirs))
    above, below = jnp.where(upper, mine, theirs), jnp.where(upper, theirs, mine)
    pack = [below[:rows], above[:rows], below[rows:], above[rows:], d2]
    mats = mats.reshape(n_tp, 4, r, per, lanes).transpose(0, 3, 1, 2, 4).reshape(n_fs, 4, r, lanes)
    mats, d1 = lax.optimization_barrier((mats, d1))
    mats = exchange(mats, "fs")

    def in_lanes(down):
        return jnp.concatenate([down[:, k * lanes : (k + 1) * lanes] for k in range(dcols // lanes)], axis=0)

    def pair_of(got):
        pair = got.reshape(n_tp, n_fs, 2, r, lanes).transpose(2, 1, 0, 3, 4).reshape(2, width, lanes)
        return pair[0], pair[1]

    def down_of(got):
        down = got.reshape(n_tp, dcols // lanes, hid, lanes)
        return down.transpose(2, 0, 1, 3).reshape(hid, width)

    d1 = in_lanes(d1)
    down = gather_tp_beside(d1)
    pack, down = lax.optimization_barrier((jnp.concatenate(pack, axis=0), down))
    whole = lax.all_gather(
        row_major(pack), "fs", axis=0, tiled=True, axis_index_groups=role_groups(n_fs)
    )
    whole = row_major(whole).reshape(n_fs // 2, 4 * rows + hid, cols // 2)
    mats, down = lax.optimization_barrier((mats, down))
    first = (*pair_of(gather_tp(mats[:, :2].reshape(-1, lanes))), down_of(down))
    rest = (mats[:, 2:].reshape(-1, lanes), d2)

    stream = prompt.astype(jnp.float32)
    normed = normed_of(stream)
    gate = jnp.dot(normed, first[0], preferred_element_type=jnp.float32)
    up = jnp.dot(normed, first[1], preferred_element_type=jnp.float32)
    hidden = (jax.nn.silu(gate) * up).astype(BF16)
    partial = jnp.dot(hidden, first[2], preferred_element_type=jnp.float32)
    tokens = prompt.shape[0] // n_fs
    own = lax.dynamic_slice_in_dim(prompt, me * tokens, tokens, 0).astype(jnp.float32)
    total, rest = scatter_sum(partial, rest, lambda pair, down: jnp.concatenate([pair, in_lanes(down)], axis=0))
    own = own + 0.5 * total
    cut = 2 * n_fs * r
    second = (*pair_of(rest[:, :cut]), down_of(rest[:, cut:]))

    both = pair_groups(n_fs, n_tp)
    members = 2 * n_tp
    normed = spread_copies(normed_of(own), ("fs", "tp"), members, both).reshape(members * tokens, width)
    hidden = spread_copies(hidden_kernel(normed, whole), "tp", n_tp)
    out = down_kernel(hidden, whole, hid)
    out = exchange(out.reshape(members, tokens, dcols), ("fs", "tp"), both)
    out = jnp.sum(out.reshape(2, n_tp, tokens, dcols), axis=0)
    own = own + 0.5 * out.transpose(1, 0, 2).reshape(tokens, width)
    result = gather_tokens(own.astype(BF16))
    return (result, first[0], first[1], first[2], second[0], second[1], second[2])


def solution(mesh):
    return jax.shard_map(
        on_device,
        mesh=mesh,
        in_specs=(
            P(("grp", "tp"), None),
            P("fs"),
            P("fs", "tp"),
            P("fs", "tp"),
            P("fs", "tp"),
            P("fs"),
            P("fs", "tp"),
            P("fs", "tp"),
            P("fs", "tp"),
        ),
        out_specs=(
            P(("grp", "tp"), None),
            P("grp", "fs"),
            P("grp", "fs"),
            P("fs", "grp"),
            P("grp", "fs"),
            P("grp", "fs"),
            P("fs", "grp"),
        ),
        check_vma=False,
    )
```

```python
import jax
import jax.numpy as jnp
from jax import lax
from jax.experimental import pallas as pl
from jax.experimental.layout import Layout, with_layout_constraint
from jax.experimental.pallas import tpu as pltpu
from jax.sharding import PartitionSpec as P


EPS = 1e-06
NEAR = 4
BF16 = jnp.bfloat16


def fold(gain, weight):
    return (gain[:, None] * weight).astype(BF16)


def normed_of(stream):
    return (stream * lax.rsqrt(jnp.mean(stream * stream, axis=-1, keepdims=True) + EPS)).astype(BF16)


def row_major(array):
    return with_layout_constraint(array, Layout(major_to_minor=tuple(range(array.ndim))))


def exchange(blocks, axis, groups=None):
    return lax.all_to_all(blocks, axis, split_axis=0, concat_axis=0, tiled=True, axis_index_groups=groups)


def spread_copies(array, axis, members, groups=None):
    copies = jnp.broadcast_to(array, (members, *array.shape))
    if groups is not None and len(groups[0]) > members:
        copies = copies.reshape(len(groups[0]), *array.shape[1:])
    return exchange(copies, axis, groups)


def far_groups(n):
    return [list(range(i, n, NEAR)) for i in range(NEAR)]


def chip_groups(n):
    return [list(range(c, n, 2)) for c in range(2)]


def gather_tp(array):
    n = lax.axis_size("tp")
    mine = spread_copies(array, "tp", n // 2, chip_groups(n))
    other = lax.ppermute(mine, "tp", [(i, i ^ 1) for i in range(n)])
    even = lax.axis_index("tp") % 2 == 0
    both = jnp.stack([jnp.where(even, mine, other), jnp.where(even, other, mine)], axis=1)
    return both.reshape(n, *array.shape)


def shift_tp(array, steps):
    n = lax.axis_size("tp")
    return lax.ppermute(array, "tp", [(i, (i + steps) % n) for i in range(n)])


def gather_tp_beside(array):
    n = lax.axis_size("tp")
    chips = n // 2
    me = lax.axis_index("tp")
    mine = jnp.zeros((chips, *array.shape), array.dtype)
    for d in range(chips):
        piece = array if d == 0 else shift_tp(array, -2 * d)
        mine = lax.dynamic_update_index_in_dim(mine, piece, (me // 2 + d) % chips, 0)
    other = lax.ppermute(mine, "tp", [(i, i ^ 1) for i in range(n)])
    even = me % 2 == 0
    both = jnp.stack([jnp.where(even, mine, other), jnp.where(even, other, mine)], axis=1)
    return both.reshape(n, *array.shape)


def shift(array, steps):
    n = lax.axis_size("fs")
    return lax.ppermute(array, "fs", [(i, (i + steps) % n) for i in range(n)])


def part_of(blocks, index, axis=0):
    return lax.dynamic_index_in_dim(blocks, index % blocks.shape[axis], axis, keepdims=False)


def scatter_sum(partial):
    n = lax.axis_size("fs")
    me = lax.axis_index("fs")
    far = n // NEAR
    rows = partial.shape[0] // n
    width = partial.shape[1]
    f32 = jnp.float32

    blocks = partial.astype(BF16).reshape(far, NEAR, rows, width)
    keep, ahead, across, behind = (part_of(blocks, me + d, 1) for d in range(NEAR))
    h = far // 2
    ahead, behind = shift(ahead, 1), shift(behind, -1)
    low, high = shift(across[:h], 2), shift(across[h:], -2)
    total = keep.astype(f32) + ahead.astype(f32) + behind.astype(f32)
    total = total + jnp.concatenate([low, high], axis=0).astype(f32)

    got = exchange(total.astype(BF16), "fs", far_groups(n))
    return jnp.sum(got.astype(f32), axis=0)


def spread_far(own):
    n = lax.axis_size("fs")
    return spread_copies(own, "fs", n // NEAR, far_groups(n))


def gather_near(got):
    n = lax.axis_size("fs")
    me = lax.axis_index("fs")
    far, rows, width = got.shape
    h = far // 2
    ahead, behind = shift(got, -1), shift(got, 1)
    low, high = shift(got[:h], 2), shift(got[h:], -2)
    out = jnp.zeros((far, NEAR, rows, width), got.dtype)
    pieces = (got, ahead, jnp.concatenate([low, high], axis=0), behind)
    for d, piece in enumerate(pieces):
        out = lax.dynamic_update_index_in_dim(out, piece, (me + d) % NEAR, 1)
    return out.reshape(n * rows, width)


def cast_in_plane(whole, rows):
    n, n_tp = lax.axis_size("fs"), lax.axis_size("tp")
    chips = n_tp // 2
    per = n // n_tp
    me, t = lax.axis_index("fs"), lax.axis_index("tp")
    planes, _, cols = whole.shape
    lanes = cols * 2 // per
    home = me // per
    ahead = (t // 2 - home // 2) % chips

    def at(f, steps, core):
        return f * n_tp + 2 * ((f // per // 2 + steps) % chips) + core

    def hop(array, pairs):
        return lax.ppermute(array, ("fs", "tp"), [pair for f in range(n) for pair in pairs(f)])

    def first():
        both = whole[:, : 4 * rows].reshape(planes, 2, 2, rows, cols)
        both = jnp.where(me % per // 2 == 0, both[:, :, 0], both[:, :, 1])
        both = jnp.where(me % 2 == 0, both[..., :lanes], both[..., lanes:])
        return both.transpose(1, 0, 2, 3).reshape(2, planes * rows, lanes)

    def second(array):
        other = hop(array, lambda f: [(f * n_tp + f // per, f * n_tp + (f // per ^ 1))])
        return lambda: jnp.where(t == home, array, other)

    def third(array):
        up = hop(array, lambda f: [(at(f, 0, c), at(f, 1, c)) for c in range(2)])
        down = hop(array, lambda f: [(at(f, 0, c), at(f, -1, c)) for c in range(2)])
        return lambda: jnp.where(ahead == 0, array, jnp.where(ahead == 1, up, down))

    def fourth(array):
        gate = hop(array[0], lambda f: [(at(f, 1, c), at(f, 2, c)) for c in range(2)])
        up = hop(array[1], lambda f: [(at(f, -1, c), at(f, -2, c)) for c in range(2)])
        return lambda: (jnp.where(ahead == 2, gate, array[0]), jnp.where(ahead == 2, up, array[1]))

    return first, second, third, fourth


STEPS = 4


def hidden_kernel(normed, whole):
    tokens, width = normed.shape
    planes, _, cols = whole.shape
    rows = width // planes
    halves = 2
    per = planes // STEPS
    group = 256 // rows

    def body(x_ref, w_ref, o_ref, acc_ref):
        step = pl.program_id(0)

        @pl.when(step == 0)
        def _():
            acc_ref[...] = jnp.zeros_like(acc_ref)

        for j in range(per // group):
            x = x_ref[:, j * group * rows : (j + 1) * group * rows]
            for m in range(2 * halves):
                w = jnp.concatenate(
                    [w_ref[j * group + k, m * rows : (m + 1) * rows, :] for k in range(group)], axis=0
                )
                acc_ref[m] += jnp.dot(x, w, preferred_element_type=jnp.float32)

        @pl.when(step == STEPS - 1)
        def _():
            for m in range(halves):
                gate, up = acc_ref[m], acc_ref[halves + m]
                o_ref[:, m * cols : (m + 1) * cols] = (gate / (1.0 + jnp.exp(-gate)) * up).astype(BF16)

    return pl.pallas_call(
        body,
        grid=(STEPS,),
        in_specs=[
            pl.BlockSpec((tokens, width // STEPS), lambda i: (0, i)),
            pl.BlockSpec((per, 2 * halves * rows, cols), lambda i: (i, 0, 0)),
        ],
        out_specs=pl.BlockSpec((tokens, halves * cols), lambda i: (0, 0)),
        out_shape=jax.ShapeDtypeStruct((tokens, halves * cols), BF16),
        scratch_shapes=[pltpu.VMEM((2 * halves, tokens, cols), jnp.float32)],
        name="hidden_second",
    )(normed, whole)


def down_kernel(hidden, whole, hid):
    n_tp, tokens, cols = hidden.shape
    planes, rows, width = whole.shape
    per = planes // STEPS
    blocks = n_tp // STEPS
    each = per // blocks

    def body(h_ref, w_ref, o_ref):
        step = pl.program_id(0)

        @pl.when(step == 0)
        def _():
            o_ref[...] = jnp.zeros_like(o_ref)

        for b in range(blocks):
            w = w_ref[b * each : (b + 1) * each].reshape(cols, width)
            o_ref[...] += jnp.dot(h_ref[b], w, preferred_element_type=jnp.float32)

    return pl.pallas_call(
        body,
        grid=(STEPS,),
        in_specs=[
            pl.BlockSpec((blocks, tokens, cols), lambda i: (i, 0, 0)),
            pl.BlockSpec((per, hid, width), lambda i: (i, rows // hid - 1, 0)),
        ],
        out_specs=pl.BlockSpec((tokens, width), lambda i: (0, 0)),
        out_shape=jax.ShapeDtypeStruct((tokens, width), jnp.float32),
        name="down_second",
    )(hidden, whole)


def on_device(
    prompt,
    gain_first,
    gate_first,
    up_first,
    down_first,
    gain_second,
    gate_second,
    up_second,
    down_second,
):
    n_fs = lax.axis_size("fs")
    n_tp = lax.axis_size("tp")
    rows, cols = gate_first.shape
    hid, dcols = down_first.shape
    width = prompt.shape[1]
    half = cols // dcols

    g1, u1 = fold(gain_first, gate_first), fold(gain_first, up_first)
    g2, u2 = fold(gain_second, gate_second), fold(gain_second, up_second)
    d1, d2 = down_first.astype(BF16), down_second.astype(BF16)

    pack = [m[:, k * dcols : (k + 1) * dcols] for m in (g2, u2) for k in range(half)] + [d2]
    whole = lax.all_gather(row_major(jnp.concatenate(pack, axis=0)), "fs", axis=0, tiled=True)
    whole = row_major(whole).reshape(n_fs, 2 * half * rows + hid, dcols)

    r = rows // n_tp
    lanes = cols * n_tp // n_fs
    per = n_fs // n_tp
    mats = jnp.stack([g1, u1]).reshape(2, n_tp, r, cols).transpose(1, 0, 2, 3)
    mats = exchange(mats, "tp")
    mats = mats.reshape(n_tp, 2, r, per, lanes).transpose(0, 3, 1, 2, 4).reshape(n_fs, 2, r, lanes)
    mats, d1, d2 = lax.optimization_barrier((mats, d1, d2))
    mats = exchange(mats, "fs")

    def in_lanes(down):
        return [down[:, k * lanes : (k + 1) * lanes] for k in range(dcols // lanes)]

    def pair_of(got):
        pair = got.reshape(n_tp, n_fs, 2, r, lanes).transpose(2, 1, 0, 3, 4).reshape(2, width, lanes)
        return pair[0], pair[1]

    def down_of(got):
        down = got.reshape(n_tp, dcols // lanes, hid, lanes)
        return down.transpose(2, 0, 1, 3).reshape(hid, width)

    downs = jnp.concatenate([*in_lanes(d1), *in_lanes(d2)], axis=0)
    downs = gather_tp_beside(downs)
    mats, downs = lax.optimization_barrier((mats, downs))
    cut = dcols // lanes * hid
    first = (*pair_of(gather_tp(mats.reshape(-1, lanes))), down_of(downs[:, :cut]))
    down_second_served = down_of(downs[:, cut:])

    stream = prompt.astype(jnp.float32)
    normed = normed_of(stream)
    gate = jnp.dot(normed, first[0], preferred_element_type=jnp.float32)
    up = jnp.dot(normed, first[1], preferred_element_type=jnp.float32)
    hidden = (jax.nn.silu(gate) * up).astype(BF16)
    partial = jnp.dot(hidden, first[2], preferred_element_type=jnp.float32)
    tokens = prompt.shape[0] // n_fs
    own = lax.dynamic_slice_in_dim(prompt, lax.axis_index("fs") * tokens, tokens, 0).astype(jnp.float32)
    own = own + 0.5 * scatter_sum(partial)

    normed = spread_copies(normed_of(own), "tp", n_tp).reshape(n_tp * tokens, width)
    hidden = hidden_kernel(normed, whole)
    step1, step2, step3, step4 = cast_in_plane(whole, rows)
    hidden = spread_copies(hidden, "tp", n_tp)
    cast = step1()
    done = step2(cast)
    out = down_kernel(hidden, whole, hid)
    out = exchange(out.reshape(n_tp, tokens, dcols), "tp")
    cast = done()
    done = step3(cast)
    own = own + 0.5 * out.transpose(1, 0, 2).reshape(tokens, width)
    got = spread_far(own.astype(BF16))
    cast = done()
    done = step4(cast)
    gate_served, up_served = done()
    result = gather_near(got)
    return (result, first[0], first[1], first[2], gate_served, up_served, down_second_served)


def solution(mesh):
    return jax.shard_map(
        on_device,
        mesh=mesh,
        in_specs=(
            P(("grp", "tp"), None),
            P("fs"),
            P("fs", "tp"),
            P("fs", "tp"),
            P("fs", "tp"),
            P("fs"),
            P("fs", "tp"),
            P("fs", "tp"),
            P("fs", "tp"),
        ),
        out_specs=(
            P(("grp", "tp"), None),
            P("grp", "fs"),
            P("grp", "fs"),
            P("fs", "grp"),
            P("grp", "fs"),
            P("grp", "fs"),
            P("fs", "grp"),
        ),
        check_vma=False,
    )
```

```python
import jax
import jax.numpy as jnp
from jax import lax
from jax.experimental import pallas as pl
from jax.experimental.layout import Layout, with_layout_constraint
from jax.experimental.pallas import tpu as pltpu
from jax.sharding import PartitionSpec as P


EPS = 1e-06
NEAR = 4
BF16 = jnp.bfloat16


def fold(gain, weight):
    return (gain[:, None] * weight).astype(BF16)


def normed_of(stream):
    return (stream * lax.rsqrt(jnp.mean(stream * stream, axis=-1, keepdims=True) + EPS)).astype(BF16)


def row_major(array):
    return with_layout_constraint(array, Layout(major_to_minor=tuple(range(array.ndim))))


def exchange(blocks, axis, groups=None):
    return lax.all_to_all(blocks, axis, split_axis=0, concat_axis=0, tiled=True, axis_index_groups=groups)


def spread_copies(array, axis, members, groups=None):
    copies = jnp.broadcast_to(array, (members, *array.shape))
    if groups is not None and len(groups[0]) > members:
        copies = copies.reshape(len(groups[0]), *array.shape[1:])
    return exchange(copies, axis, groups)


def far_groups(n):
    return [list(range(i, n, NEAR)) for i in range(NEAR)]


def chip_groups(n):
    return [list(range(c, n, 2)) for c in range(2)]


def gather_tp(array):
    n = lax.axis_size("tp")
    mine = spread_copies(array, "tp", n // 2, chip_groups(n))
    other = lax.ppermute(mine, "tp", [(i, i ^ 1) for i in range(n)])
    even = lax.axis_index("tp") % 2 == 0
    both = jnp.stack([jnp.where(even, mine, other), jnp.where(even, other, mine)], axis=1)
    return both.reshape(n, *array.shape)


def shift_tp(array, steps):
    n = lax.axis_size("tp")
    return lax.ppermute(array, "tp", [(i, (i + steps) % n) for i in range(n)])


def gather_tp_beside(array):
    n = lax.axis_size("tp")
    chips = n // 2
    me = lax.axis_index("tp")
    mine = jnp.zeros((chips, *array.shape), array.dtype)
    for d in range(chips):
        piece = array if d == 0 else shift_tp(array, -2 * d)
        mine = lax.dynamic_update_index_in_dim(mine, piece, (me // 2 + d) % chips, 0)
    other = lax.ppermute(mine, "tp", [(i, i ^ 1) for i in range(n)])
    even = me % 2 == 0
    both = jnp.stack([jnp.where(even, mine, other), jnp.where(even, other, mine)], axis=1)
    return both.reshape(n, *array.shape)


def shift(array, steps):
    n = lax.axis_size("fs")
    return lax.ppermute(array, "fs", [(i, (i + steps) % n) for i in range(n)])


def part_of(blocks, index, axis=0):
    return lax.dynamic_index_in_dim(blocks, index % blocks.shape[axis], axis, keepdims=False)


def scatter_sum(partial):
    n = lax.axis_size("fs")
    me = lax.axis_index("fs")
    far = n // NEAR
    rows = partial.shape[0] // n
    width = partial.shape[1]
    f32 = jnp.float32

    blocks = partial.astype(BF16).reshape(far, NEAR, rows, width)
    keep, ahead, across, behind = (part_of(blocks, me + d, 1) for d in range(NEAR))
    h = far // 2
    ahead, behind = shift(ahead, 1), shift(behind, -1)
    low, high = shift(across[:h], 2), shift(across[h:], -2)
    total = keep.astype(f32) + ahead.astype(f32) + behind.astype(f32)
    total = total + jnp.concatenate([low, high], axis=0).astype(f32)

    got = exchange(total.astype(BF16), "fs", far_groups(n))
    return jnp.sum(got.astype(f32), axis=0)


def spread_far(own):
    n = lax.axis_size("fs")
    return spread_copies(own, "fs", n // NEAR, far_groups(n))


def gather_near(got):
    n = lax.axis_size("fs")
    me = lax.axis_index("fs")
    far, rows, width = got.shape
    h = far // 2
    ahead, behind = shift(got, -1), shift(got, 1)
    low, high = shift(got[:h], 2), shift(got[h:], -2)
    out = jnp.zeros((far, NEAR, rows, width), got.dtype)
    pieces = (got, ahead, jnp.concatenate([low, high], axis=0), behind)
    for d, piece in enumerate(pieces):
        out = lax.dynamic_update_index_in_dim(out, piece, (me + d) % NEAR, 1)
    return out.reshape(n * rows, width)


def cast_in_plane(whole, rows):
    n, n_tp = lax.axis_size("fs"), lax.axis_size("tp")
    chips = n_tp // 2
    per = n // n_tp
    me, t = lax.axis_index("fs"), lax.axis_index("tp")
    planes, _, cols = whole.shape
    lanes = cols * 2 // per
    home = me // per
    ahead = (t // 2 - home // 2) % chips

    def at(f, steps, core):
        return f * n_tp + 2 * ((f // per // 2 + steps) % chips) + core

    def hop(array, pairs):
        return lax.ppermute(array, ("fs", "tp"), [pair for f in range(n) for pair in pairs(f)])

    def first():
        half = me % per // 2 * rows
        both = [lax.dynamic_slice(whole, (0, 2 * m * rows + half, 0), (planes, rows, cols)) for m in range(2)]
        both = [jnp.where(me % 2 == 0, w[..., :lanes], w[..., lanes:]) for w in both]
        return jnp.stack([w.reshape(planes * rows, lanes) for w in both])

    def second(array):
        other = hop(array, lambda f: [(f * n_tp + f // per, f * n_tp + (f // per ^ 1))])
        return lambda: jnp.where(t == home, array, other)

    def third(array):
        up = hop(array, lambda f: [(at(f, 0, c), at(f, 1, c)) for c in range(2)])
        down = hop(array, lambda f: [(at(f, 0, c), at(f, -1, c)) for c in range(2)])
        return lambda: jnp.where(ahead == 0, array, jnp.where(ahead == 1, up, down))

    def fourth(array):
        gate = hop(array[0], lambda f: [(at(f, 1, c), at(f, 2, c)) for c in range(2)])
        up = hop(array[1], lambda f: [(at(f, -1, c), at(f, -2, c)) for c in range(2)])
        return lambda: (jnp.where(ahead == 2, gate, array[0]), jnp.where(ahead == 2, up, array[1]))

    return first, second, third, fourth


STEPS = 4


def hidden_kernel(normed, whole):
    tokens, width = normed.shape
    planes, _, cols = whole.shape
    rows = width // planes
    halves = 2
    per = planes // STEPS
    group = 256 // rows

    def body(x_ref, w_ref, o_ref, acc_ref):
        step = pl.program_id(0)

        @pl.when(step == 0)
        def _():
            acc_ref[...] = jnp.zeros_like(acc_ref)

        for j in range(per // group):
            x = x_ref[:, j * group * rows : (j + 1) * group * rows]
            for m in range(2 * halves):
                w = jnp.concatenate(
                    [w_ref[j * group + k, m * rows : (m + 1) * rows, :] for k in range(group)], axis=0
                )
                acc_ref[m] += jnp.dot(x, w, preferred_element_type=jnp.float32)

        @pl.when(step == STEPS - 1)
        def _():
            for m in range(halves):
                gate, up = acc_ref[m], acc_ref[halves + m]
                o_ref[:, m * cols : (m + 1) * cols] = (gate / (1.0 + jnp.exp(-gate)) * up).astype(BF16)

    return pl.pallas_call(
        body,
        grid=(STEPS,),
        in_specs=[
            pl.BlockSpec((tokens, width // STEPS), lambda i: (0, i)),
            pl.BlockSpec((per, 2 * halves * rows, cols), lambda i: (i, 0, 0)),
        ],
        out_specs=pl.BlockSpec((tokens, halves * cols), lambda i: (0, 0)),
        out_shape=jax.ShapeDtypeStruct((tokens, halves * cols), BF16),
        scratch_shapes=[pltpu.VMEM((2 * halves, tokens, cols), jnp.float32)],
        name="hidden_second",
    )(normed, whole)


def down_kernel(hidden, whole, hid):
    n_tp, tokens, cols = hidden.shape
    planes, rows, width = whole.shape
    per = planes // STEPS
    blocks = n_tp // STEPS
    each = per // blocks

    def body(h_ref, w_ref, o_ref):
        step = pl.program_id(0)

        @pl.when(step == 0)
        def _():
            o_ref[...] = jnp.zeros_like(o_ref)

        for b in range(blocks):
            w = w_ref[b * each : (b + 1) * each].reshape(cols, width)
            o_ref[...] += jnp.dot(h_ref[b], w, preferred_element_type=jnp.float32)

    return pl.pallas_call(
        body,
        grid=(STEPS,),
        in_specs=[
            pl.BlockSpec((blocks, tokens, cols), lambda i: (i, 0, 0)),
            pl.BlockSpec((per, hid, width), lambda i: (i, rows // hid - 1, 0)),
        ],
        out_specs=pl.BlockSpec((tokens, width), lambda i: (0, 0)),
        out_shape=jax.ShapeDtypeStruct((tokens, width), jnp.float32),
        name="down_second",
    )(hidden, whole)


def on_device(
    prompt,
    gain_first,
    gate_first,
    up_first,
    down_first,
    gain_second,
    gate_second,
    up_second,
    down_second,
):
    n_fs = lax.axis_size("fs")
    n_tp = lax.axis_size("tp")
    rows, cols = gate_first.shape
    hid, dcols = down_first.shape
    width = prompt.shape[1]
    half = cols // dcols

    g1, u1 = fold(gain_first, gate_first), fold(gain_first, up_first)
    g2, u2 = fold(gain_second, gate_second), fold(gain_second, up_second)
    d1, d2 = down_first.astype(BF16), down_second.astype(BF16)

    pack = [m[:, k * dcols : (k + 1) * dcols] for m in (g2, u2) for k in range(half)] + [d2]
    whole = lax.all_gather(row_major(jnp.concatenate(pack, axis=0)), "fs", axis=0, tiled=True)
    whole = row_major(whole).reshape(n_fs, 2 * half * rows + hid, dcols)

    r = rows // n_tp
    lanes = cols * n_tp // n_fs
    per = n_fs // n_tp
    mats = jnp.stack([g1, u1]).reshape(2, n_tp, r, cols).transpose(1, 0, 2, 3)
    mats = exchange(mats, "tp")
    mats = mats.reshape(n_tp, 2, r, per, lanes).transpose(0, 3, 1, 2, 4).reshape(n_fs, 2, r, lanes)
    mats, d1, d2 = lax.optimization_barrier((mats, d1, d2))
    mats = exchange(mats, "fs")

    def in_lanes(down):
        return [down[:, k * lanes : (k + 1) * lanes] for k in range(dcols // lanes)]

    def pair_of(got):
        pair = got.reshape(n_tp, n_fs, 2, r, lanes).transpose(2, 1, 0, 3, 4).reshape(2, width, lanes)
        return pair[0], pair[1]

    def down_of(got):
        down = got.reshape(n_tp, dcols // lanes, hid, lanes)
        return down.transpose(2, 0, 1, 3).reshape(hid, width)

    downs = jnp.concatenate([*in_lanes(d1), *in_lanes(d2)], axis=0)
    downs = gather_tp_beside(downs)
    mats, downs = lax.optimization_barrier((mats, downs))
    cut = dcols // lanes * hid
    first = (*pair_of(gather_tp(mats.reshape(-1, lanes))), down_of(downs[:, :cut]))
    down_second_served = down_of(downs[:, cut:])

    stream = prompt.astype(jnp.float32)
    normed = normed_of(stream)
    gate = jnp.dot(normed, first[0], preferred_element_type=jnp.float32)
    up = jnp.dot(normed, first[1], preferred_element_type=jnp.float32)
    hidden = (jax.nn.silu(gate) * up).astype(BF16)
    partial = jnp.dot(hidden, first[2], preferred_element_type=jnp.float32)
    tokens = prompt.shape[0] // n_fs
    own = lax.dynamic_slice_in_dim(prompt, lax.axis_index("fs") * tokens, tokens, 0).astype(jnp.float32)
    own = own + 0.5 * scatter_sum(partial)

    normed = spread_copies(normed_of(own), "tp", n_tp).reshape(n_tp * tokens, width)
    hidden = hidden_kernel(normed, whole)
    step1, step2, step3, step4 = cast_in_plane(whole, rows)
    hidden = spread_copies(hidden, "tp", n_tp)
    cast = step1()
    done = step2(cast)
    out = down_kernel(hidden, whole, hid)
    out = exchange(out.reshape(n_tp, tokens, dcols), "tp")
    cast = done()
    done = step3(cast)
    own = own + 0.5 * out.transpose(1, 0, 2).reshape(tokens, width)
    got = spread_far(own.astype(BF16))
    cast = done()
    done = step4(cast)
    gate_served, up_served = done()
    result = gather_near(got)
    return (result, first[0], first[1], first[2], gate_served, up_served, down_second_served)


def solution(mesh):
    return jax.shard_map(
        on_device,
        mesh=mesh,
        in_specs=(
            P(("grp", "tp"), None),
            P("fs"),
            P("fs", "tp"),
            P("fs", "tp"),
            P("fs", "tp"),
            P("fs"),
            P("fs", "tp"),
            P("fs", "tp"),
            P("fs", "tp"),
        ),
        out_specs=(
            P(("grp", "tp"), None),
            P("grp", "fs"),
            P("grp", "fs"),
            P("fs", "grp"),
            P("grp", "fs"),
            P("grp", "fs"),
            P("fs", "grp"),
        ),
        check_vma=False,
    )
```

```python
import jax
import jax.numpy as jnp
from jax import lax
from jax.experimental import pallas as pl
from jax.experimental.layout import Layout, with_layout_constraint
from jax.experimental.pallas import tpu as pltpu
from jax.sharding import PartitionSpec as P


EPS = 1e-06
NEAR = 4
BF16 = jnp.bfloat16


def fold(gain, weight):
    return (gain[:, None] * weight).astype(BF16)


def normed_of(stream):
    return (stream * lax.rsqrt(jnp.mean(stream * stream, axis=-1, keepdims=True) + EPS)).astype(BF16)


def row_major(array):
    return with_layout_constraint(array, Layout(major_to_minor=tuple(range(array.ndim))))


def exchange(blocks, axis, groups=None):
    return lax.all_to_all(blocks, axis, split_axis=0, concat_axis=0, tiled=True, axis_index_groups=groups)


def spread_copies(array, axis, members, groups=None):
    copies = jnp.broadcast_to(array, (members, *array.shape))
    if groups is not None and len(groups[0]) > members:
        copies = copies.reshape(len(groups[0]), *array.shape[1:])
    return exchange(copies, axis, groups)


def far_groups(n):
    return [list(range(i, n, NEAR)) for i in range(NEAR)]


def chip_groups(n):
    return [list(range(c, n, 2)) for c in range(2)]


def gather_tp(array):
    n = lax.axis_size("tp")
    mine = spread_copies(array, "tp", n // 2, chip_groups(n))
    other = lax.ppermute(mine, "tp", [(i, i ^ 1) for i in range(n)])
    even = lax.axis_index("tp") % 2 == 0
    both = jnp.stack([jnp.where(even, mine, other), jnp.where(even, other, mine)], axis=1)
    return both.reshape(n, *array.shape)


def shift_tp(array, steps):
    n = lax.axis_size("tp")
    return lax.ppermute(array, "tp", [(i, (i + steps) % n) for i in range(n)])


def gather_tp_beside(array):
    n = lax.axis_size("tp")
    chips = n // 2
    me = lax.axis_index("tp")
    mine = jnp.zeros((chips, *array.shape), array.dtype)
    for d in range(chips):
        piece = array if d == 0 else shift_tp(array, -2 * d)
        mine = lax.dynamic_update_index_in_dim(mine, piece, (me // 2 + d) % chips, 0)
    other = lax.ppermute(mine, "tp", [(i, i ^ 1) for i in range(n)])
    even = me % 2 == 0
    both = jnp.stack([jnp.where(even, mine, other), jnp.where(even, other, mine)], axis=1)
    return both.reshape(n, *array.shape)


def shift(array, steps):
    n = lax.axis_size("fs")
    return lax.ppermute(array, "fs", [(i, (i + steps) % n) for i in range(n)])


def part_of(blocks, index, axis=0):
    return lax.dynamic_index_in_dim(blocks, index % blocks.shape[axis], axis, keepdims=False)


def scatter_sum(partial):
    n = lax.axis_size("fs")
    me = lax.axis_index("fs")
    far = n // NEAR
    rows = partial.shape[0] // n
    width = partial.shape[1]
    f32 = jnp.float32

    blocks = partial.astype(BF16).reshape(far, NEAR, rows, width)
    keep, ahead, across, behind = (part_of(blocks, me + d, 1) for d in range(NEAR))
    h = far // 2
    ahead, behind = shift(ahead, 1), shift(behind, -1)
    low, high = shift(across[:h], 2), shift(across[h:], -2)
    total = keep.astype(f32) + ahead.astype(f32) + behind.astype(f32)
    total = total + jnp.concatenate([low, high], axis=0).astype(f32)

    got = exchange(total.astype(BF16), "fs", far_groups(n))
    return jnp.sum(got.astype(f32), axis=0)


def spread_far(own):
    n = lax.axis_size("fs")
    return spread_copies(own, "fs", n // NEAR, far_groups(n))


def gather_near(got):
    n = lax.axis_size("fs")
    me = lax.axis_index("fs")
    far, rows, width = got.shape
    h = far // 2
    ahead = shift(got, -1)
    behind = shift(got, 1)
    low, high = shift(got[:h], 2), shift(got[h:], -2)
    out = jnp.zeros((far, NEAR, rows, width), got.dtype)
    pieces = (got, ahead, jnp.concatenate([low, high], axis=0), behind)
    for d, piece in enumerate(pieces):
        out = lax.dynamic_update_index_in_dim(out, piece, (me + d) % NEAR, 1)
    return out.reshape(n * rows, width)


def cast_in_plane(whole, rows):
    n, n_tp = lax.axis_size("fs"), lax.axis_size("tp")
    chips = n_tp // 2
    per = n // n_tp
    me, t = lax.axis_index("fs"), lax.axis_index("tp")
    core = t % 2
    planes, _, cols = whole.shape
    lanes = cols * 2 // per
    home = me // per
    ahead = (t // 2 - home // 2) % chips

    def at(f, steps, core):
        return f * n_tp + 2 * ((f // per // 2 + steps) % chips) + core

    def hop(array, pairs):
        return lax.ppermute(array, ("fs", "tp"), [pair for f in range(n) for pair in pairs(f)])

    def first():
        half = me % per // 2 * rows
        both = [lax.dynamic_slice(whole, (0, 2 * m * rows + half, 0), (planes, rows, cols)) for m in range(2)]
        both = [jnp.where(me % 2 == 0, w[..., :lanes], w[..., lanes:]).reshape(planes * rows, lanes) for w in both]
        return jnp.where(core == 0, both[0], both[1]), jnp.where(core == 0, both[1], both[0])

    def second(mine, theirs):
        other = hop(theirs, lambda f: [(f * n_tp + f // per, f * n_tp + (f // per ^ 1))])
        return lambda: jnp.where(t == home, mine, other)

    def third(mine):
        up = hop(mine, lambda f: [(at(f, 0, c), at(f, 1, c)) for c in range(2)])
        down = hop(mine, lambda f: [(at(f, 0, c), at(f, -1, c)) for c in range(2)])
        return lambda: jnp.where(ahead == 0, mine, jnp.where(ahead == 1, up, down))

    def fourth(mine):
        h = mine.shape[0] // 2
        low = hop(mine[:h], lambda f: [(at(f, 1, c), at(f, 2, c)) for c in range(2)])
        high = hop(mine[h:], lambda f: [(at(f, -1, c), at(f, -2, c)) for c in range(2)])
        return lambda: jnp.where(ahead == 2, jnp.concatenate([low, high], axis=0), mine)

    def fifth(mine):
        other = hop(mine, lambda f: [(f * n_tp + t, f * n_tp + (t ^ 1)) for t in range(n_tp)])
        return lambda: (jnp.where(core == 0, mine, other), jnp.where(core == 0, other, mine))

    return first, second, third, fourth, fifth


STEPS = 4


def hidden_kernel(normed, whole):
    tokens, width = normed.shape
    planes, _, cols = whole.shape
    rows = width // planes
    halves = 2
    per = planes // STEPS
    group = 256 // rows

    def body(x_ref, w_ref, o_ref, acc_ref):
        step = pl.program_id(0)

        @pl.when(step == 0)
        def _():
            acc_ref[...] = jnp.zeros_like(acc_ref)

        for j in range(per // group):
            x = x_ref[:, j * group * rows : (j + 1) * group * rows]
            for m in range(2 * halves):
                w = jnp.concatenate(
                    [w_ref[j * group + k, m * rows : (m + 1) * rows, :] for k in range(group)], axis=0
                )
                acc_ref[m] += jnp.dot(x, w, preferred_element_type=jnp.float32)

        @pl.when(step == STEPS - 1)
        def _():
            for m in range(halves):
                gate, up = acc_ref[m], acc_ref[halves + m]
                o_ref[:, m * cols : (m + 1) * cols] = (gate / (1.0 + jnp.exp(-gate)) * up).astype(BF16)

    return pl.pallas_call(
        body,
        grid=(STEPS,),
        in_specs=[
            pl.BlockSpec((tokens, width // STEPS), lambda i: (0, i)),
            pl.BlockSpec((per, 2 * halves * rows, cols), lambda i: (i, 0, 0)),
        ],
        out_specs=pl.BlockSpec((tokens, halves * cols), lambda i: (0, 0)),
        out_shape=jax.ShapeDtypeStruct((tokens, halves * cols), BF16),
        scratch_shapes=[pltpu.VMEM((2 * halves, tokens, cols), jnp.float32)],
        name="hidden_second",
    )(normed, whole)


def down_kernel(hidden, whole, hid):
    n_tp, tokens, cols = hidden.shape
    planes, rows, width = whole.shape
    per = planes // STEPS
    blocks = n_tp // STEPS
    each = per // blocks

    def body(h_ref, w_ref, o_ref):
        step = pl.program_id(0)

        @pl.when(step == 0)
        def _():
            o_ref[...] = jnp.zeros_like(o_ref)

        for b in range(blocks):
            w = w_ref[b * each : (b + 1) * each].reshape(cols, width)
            o_ref[...] += jnp.dot(h_ref[b], w, preferred_element_type=jnp.float32)

    return pl.pallas_call(
        body,
        grid=(STEPS,),
        in_specs=[
            pl.BlockSpec((blocks, tokens, cols), lambda i: (i, 0, 0)),
            pl.BlockSpec((per, hid, width), lambda i: (i, rows // hid - 1, 0)),
        ],
        out_specs=pl.BlockSpec((tokens, width), lambda i: (0, 0)),
        out_shape=jax.ShapeDtypeStruct((tokens, width), jnp.float32),
        name="down_second",
    )(hidden, whole)


def on_device(
    prompt,
    gain_first,
    gate_first,
    up_first,
    down_first,
    gain_second,
    gate_second,
    up_second,
    down_second,
):
    n_fs = lax.axis_size("fs")
    n_tp = lax.axis_size("tp")
    rows, cols = gate_first.shape
    hid, dcols = down_first.shape
    width = prompt.shape[1]
    half = cols // dcols

    g1, u1 = fold(gain_first, gate_first), fold(gain_first, up_first)
    g2, u2 = fold(gain_second, gate_second), fold(gain_second, up_second)
    d1, d2 = down_first.astype(BF16), down_second.astype(BF16)

    pack = [m[:, k * dcols : (k + 1) * dcols] for m in (g2, u2) for k in range(half)] + [d2]
    whole = lax.all_gather(row_major(jnp.concatenate(pack, axis=0)), "fs", axis=0, tiled=True)
    whole = row_major(whole).reshape(n_fs, 2 * half * rows + hid, dcols)

    r = rows // n_tp
    lanes = cols * n_tp // n_fs
    per = n_fs // n_tp
    mats = jnp.stack([g1, u1]).reshape(2, n_tp, r, cols).transpose(1, 0, 2, 3)
    mats = exchange(mats, "tp")
    mats = mats.reshape(n_tp, 2, r, per, lanes).transpose(0, 3, 1, 2, 4).reshape(n_fs, 2, r, lanes)
    mats, d1, d2 = lax.optimization_barrier((mats, d1, d2))
    mats = exchange(mats, "fs")

    def in_lanes(down):
        return [down[:, k * lanes : (k + 1) * lanes] for k in range(dcols // lanes)]

    def pair_of(got):
        pair = got.reshape(n_tp, n_fs, 2, r, lanes).transpose(2, 1, 0, 3, 4).reshape(2, width, lanes)
        return pair[0], pair[1]

    def down_of(got):
        down = got.reshape(n_tp, dcols // lanes, hid, lanes)
        return down.transpose(2, 0, 1, 3).reshape(hid, width)

    downs = jnp.concatenate([*in_lanes(d1), *in_lanes(d2)], axis=0)
    downs = gather_tp_beside(downs)
    mats, downs = lax.optimization_barrier((mats, downs))
    cut = dcols // lanes * hid
    first = (*pair_of(gather_tp(mats.reshape(-1, lanes))), down_of(downs[:, :cut]))
    down_second_served = down_of(downs[:, cut:])

    stream = prompt.astype(jnp.float32)
    normed = normed_of(stream)
    gate = jnp.dot(normed, first[0], preferred_element_type=jnp.float32)
    up = jnp.dot(normed, first[1], preferred_element_type=jnp.float32)
    hidden = (jax.nn.silu(gate) * up).astype(BF16)
    partial = jnp.dot(hidden, first[2], preferred_element_type=jnp.float32)
    tokens = prompt.shape[0] // n_fs
    own = lax.dynamic_slice_in_dim(prompt, lax.axis_index("fs") * tokens, tokens, 0).astype(jnp.float32)
    own = own + 0.5 * scatter_sum(partial)

    normed = spread_copies(normed_of(own), "tp", n_tp).reshape(n_tp * tokens, width)
    hidden = hidden_kernel(normed, whole)
    step1, step2, step3, step4, step5 = cast_in_plane(whole, rows)
    hidden = spread_copies(hidden, "tp", n_tp)
    cast = step1()
    done = step2(*cast)
    out = down_kernel(hidden, whole, hid)
    out = exchange(out.reshape(n_tp, tokens, dcols), "tp")
    cast = done()
    done = step3(cast)
    own = own + 0.5 * out.transpose(1, 0, 2).reshape(tokens, width)
    got = spread_far(own.astype(BF16))
    cast = done()
    done = step4(cast)
    result = gather_near(got)
    cast = done()
    done = step5(cast)
    gate_served, up_served = done()
    return (result, first[0], first[1], first[2], gate_served, up_served, down_second_served)


def solution(mesh):
    return jax.shard_map(
        on_device,
        mesh=mesh,
        in_specs=(
            P(("grp", "tp"), None),
            P("fs"),
            P("fs", "tp"),
            P("fs", "tp"),
            P("fs", "tp"),
            P("fs"),
            P("fs", "tp"),
            P("fs", "tp"),
            P("fs", "tp"),
        ),
        out_specs=(
            P(("grp", "tp"), None),
            P("grp", "fs"),
            P("grp", "fs"),
            P("fs", "grp"),
            P("grp", "fs"),
            P("grp", "fs"),
            P("fs", "grp"),
        ),
        check_vma=False,
    )
```

```python
import jax
import jax.numpy as jnp
from jax import lax
from jax.experimental import pallas as pl
from jax.experimental.layout import Layout, with_layout_constraint
from jax.experimental.pallas import tpu as pltpu
from jax.sharding import PartitionSpec as P


EPS = 1e-06
NEAR = 4
BF16 = jnp.bfloat16


def fold(gain, weight):
    return (gain[:, None] * weight).astype(BF16)


def normed_of(stream):
    return (stream * lax.rsqrt(jnp.mean(stream * stream, axis=-1, keepdims=True) + EPS)).astype(BF16)


def row_major(array):
    return with_layout_constraint(array, Layout(major_to_minor=tuple(range(array.ndim))))


def exchange(blocks, axis, groups=None):
    return lax.all_to_all(blocks, axis, split_axis=0, concat_axis=0, tiled=True, axis_index_groups=groups)


def spread_copies(array, axis, members, groups=None):
    copies = jnp.broadcast_to(array, (members, *array.shape))
    if groups is not None and len(groups[0]) > members:
        copies = copies.reshape(len(groups[0]), *array.shape[1:])
    return exchange(copies, axis, groups)


def far_groups(n, stride=NEAR):
    return [list(range(i, n, stride)) for i in range(stride)]


def chip_groups(n):
    return [list(range(c, n, 2)) for c in range(2)]


def gather_tp(array):
    n = lax.axis_size("tp")
    mine = spread_copies(array, "tp", n // 2, chip_groups(n))
    other = lax.ppermute(mine, "tp", [(i, i ^ 1) for i in range(n)])
    even = lax.axis_index("tp") % 2 == 0
    both = jnp.stack([jnp.where(even, mine, other), jnp.where(even, other, mine)], axis=1)
    return both.reshape(n, *array.shape)


def shift_tp(array, steps):
    n = lax.axis_size("tp")
    return lax.ppermute(array, "tp", [(i, (i + steps) % n) for i in range(n)])


def gather_tp_beside(array):
    n = lax.axis_size("tp")
    chips = n // 2
    me = lax.axis_index("tp")
    mine = jnp.zeros((chips, *array.shape), array.dtype)
    for d in range(chips):
        piece = array if d == 0 else shift_tp(array, -2 * d)
        mine = lax.dynamic_update_index_in_dim(mine, piece, (me // 2 + d) % chips, 0)
    other = lax.ppermute(mine, "tp", [(i, i ^ 1) for i in range(n)])
    even = me % 2 == 0
    both = jnp.stack([jnp.where(even, mine, other), jnp.where(even, other, mine)], axis=1)
    return both.reshape(n, *array.shape)


def shift(array, steps):
    n = lax.axis_size("fs")
    return lax.ppermute(array, "fs", [(i, (i + steps) % n) for i in range(n)])


def part_of(blocks, index, axis=0):
    return lax.dynamic_index_in_dim(blocks, index % blocks.shape[axis], axis, keepdims=False)


def scatter_sum(partial):
    n = lax.axis_size("fs")
    me = lax.axis_index("fs")
    far = n // NEAR
    rows = partial.shape[0] // n
    width = partial.shape[1]
    f32 = jnp.float32

    blocks = partial.astype(BF16).reshape(far, NEAR, rows, width)
    keep, ahead, across, behind = (part_of(blocks, me + d, 1) for d in range(NEAR))
    h = far // 2
    ahead, behind = shift(ahead, 1), shift(behind, -1)
    low, high = shift(across[:h], 2), shift(across[h:], -2)
    total = keep.astype(f32) + ahead.astype(f32) + behind.astype(f32)
    total = total + jnp.concatenate([low, high], axis=0).astype(f32)

    blocks = total.astype(BF16).reshape(far // 2, 2, rows, width)
    side = me // NEAR
    keep, other = part_of(blocks, side, 1), part_of(blocks, side + 1, 1)
    h = far // 4
    low, high = shift(other[:h], NEAR), shift(other[h:], -NEAR)
    total = keep.astype(f32) + jnp.concatenate([low, high], axis=0).astype(f32)

    got = exchange(total.astype(BF16), "fs", far_groups(n, 2 * NEAR))
    return jnp.sum(got.astype(f32), axis=0)


def spread_far(own):
    n = lax.axis_size("fs")
    return spread_copies(own, "fs", n // NEAR, far_groups(n))


def gather_near(got):
    n = lax.axis_size("fs")
    me = lax.axis_index("fs")
    far, rows, width = got.shape
    h = far // 2
    ahead, behind = shift(got, -1), shift(got, 1)
    low, high = shift(got[:h], 2), shift(got[h:], -2)
    out = jnp.zeros((far, NEAR, rows, width), got.dtype)
    pieces = (got, ahead, jnp.concatenate([low, high], axis=0), behind)
    for d, piece in enumerate(pieces):
        out = lax.dynamic_update_index_in_dim(out, piece, (me + d) % NEAR, 1)
    return out.reshape(n * rows, width)


def cast_in_plane(whole, rows):
    n, n_tp = lax.axis_size("fs"), lax.axis_size("tp")
    chips = n_tp // 2
    per = n // n_tp
    me, t = lax.axis_index("fs"), lax.axis_index("tp")
    planes, _, cols = whole.shape
    lanes = cols * 2 // per
    home = me // per
    ahead = (t // 2 - home // 2) % chips

    def at(f, steps, core):
        return f * n_tp + 2 * ((f // per // 2 + steps) % chips) + core

    def hop(array, pairs):
        return lax.ppermute(array, ("fs", "tp"), [pair for f in range(n) for pair in pairs(f)])

    def first():
        half = me % per // 2 * rows
        both = [lax.dynamic_slice(whole, (0, 2 * m * rows + half, 0), (planes, rows, cols)) for m in range(2)]
        both = [jnp.where(me % 2 == 0, w[..., :lanes], w[..., lanes:]) for w in both]
        return jnp.stack([w.reshape(planes * rows, lanes) for w in both])

    def second(array):
        other = hop(array, lambda f: [(f * n_tp + f // per, f * n_tp + (f // per ^ 1))])
        return lambda: jnp.where(t == home, array, other)

    def third(array):
        up = hop(array, lambda f: [(at(f, 0, c), at(f, 1, c)) for c in range(2)])
        down = hop(array, lambda f: [(at(f, 0, c), at(f, -1, c)) for c in range(2)])
        return lambda: jnp.where(ahead == 0, array, jnp.where(ahead == 1, up, down))

    def fourth(array):
        gate = hop(array[0], lambda f: [(at(f, 1, c), at(f, 2, c)) for c in range(2)])
        up = hop(array[1], lambda f: [(at(f, -1, c), at(f, -2, c)) for c in range(2)])
        return lambda: (jnp.where(ahead == 2, gate, array[0]), jnp.where(ahead == 2, up, array[1]))

    return first, second, third, fourth


STEPS = 4


def hidden_kernel(normed, whole, copies):
    tokens, width = normed.shape
    planes, _, cols = whole.shape
    rows = width // planes
    halves = 2
    per = planes // STEPS
    group = 256 // rows

    def body(x_ref, w_ref, o_ref, acc_ref):
        step = pl.program_id(0)

        @pl.when(step == 0)
        def _():
            acc_ref[...] = jnp.zeros_like(acc_ref)

        for j in range(per // group):
            x = x_ref[:, j * group * rows : (j + 1) * group * rows]
            for m in range(2 * halves):
                w = jnp.concatenate(
                    [w_ref[j * group + k, m * rows : (m + 1) * rows, :] for k in range(group)], axis=0
                )
                acc_ref[m] += jnp.dot(x, w, preferred_element_type=jnp.float32)

        @pl.when(step == STEPS - 1)
        def _():
            for m in range(halves):
                gate, up = acc_ref[m], acc_ref[halves + m]
                value = (gate / (1.0 + jnp.exp(-gate)) * up).astype(BF16)
                for c in range(copies):
                    o_ref[c, :, m * cols : (m + 1) * cols] = value

    return pl.pallas_call(
        body,
        grid=(STEPS,),
        in_specs=[
            pl.BlockSpec((tokens, width // STEPS), lambda i: (0, i)),
            pl.BlockSpec((per, 2 * halves * rows, cols), lambda i: (i, 0, 0)),
        ],
        out_specs=pl.BlockSpec((copies, tokens, halves * cols), lambda i: (0, 0, 0)),
        out_shape=jax.ShapeDtypeStruct((copies, tokens, halves * cols), BF16),
        scratch_shapes=[pltpu.VMEM((2 * halves, tokens, cols), jnp.float32)],
        name="hidden_second",
    )(normed, whole)


def down_kernel(hidden, whole, hid):
    n_tp, tokens, cols = hidden.shape
    planes, rows, width = whole.shape
    per = planes // STEPS
    blocks = n_tp // STEPS
    each = per // blocks

    def body(h_ref, w_ref, o_ref):
        step = pl.program_id(0)

        @pl.when(step == 0)
        def _():
            o_ref[...] = jnp.zeros_like(o_ref)

        for b in range(blocks):
            w = w_ref[b * each : (b + 1) * each].reshape(cols, width)
            o_ref[...] += jnp.dot(h_ref[b], w, preferred_element_type=jnp.float32)

    return pl.pallas_call(
        body,
        grid=(STEPS,),
        in_specs=[
            pl.BlockSpec((blocks, tokens, cols), lambda i: (i, 0, 0)),
            pl.BlockSpec((per, hid, width), lambda i: (i, rows // hid - 1, 0)),
        ],
        out_specs=pl.BlockSpec((tokens, width), lambda i: (0, 0)),
        out_shape=jax.ShapeDtypeStruct((tokens, width), jnp.float32),
        name="down_second",
    )(hidden, whole)


def on_device(
    prompt,
    gain_first,
    gate_first,
    up_first,
    down_first,
    gain_second,
    gate_second,
    up_second,
    down_second,
):
    n_fs = lax.axis_size("fs")
    n_tp = lax.axis_size("tp")
    rows, cols = gate_first.shape
    hid, dcols = down_first.shape
    width = prompt.shape[1]
    half = cols // dcols

    g1, u1 = fold(gain_first, gate_first), fold(gain_first, up_first)
    g2, u2 = fold(gain_second, gate_second), fold(gain_second, up_second)
    d1, d2 = down_first.astype(BF16), down_second.astype(BF16)

    pack = [m[:, k * dcols : (k + 1) * dcols] for m in (g2, u2) for k in range(half)] + [d2]
    pack = jnp.concatenate(pack, axis=0)
    whole = lax.all_gather(row_major(pack), "fs", axis=0, tiled=True)
    whole = row_major(whole).reshape(n_fs, 2 * half * rows + hid, dcols)

    r = rows // n_tp
    lanes = cols * n_tp // n_fs
    per = n_fs // n_tp
    mats = jnp.stack([g1, u1]).reshape(2, n_tp, r, cols).transpose(1, 0, 2, 3)
    mats = exchange(mats, "tp")
    mats = mats.reshape(n_tp, 2, r, per, lanes).transpose(0, 3, 1, 2, 4).reshape(n_fs, 2, r, lanes)
    mats, d1, d2 = lax.optimization_barrier((mats, d1, d2))
    mats = exchange(mats, "fs")

    def in_lanes(down):
        return [down[:, k * lanes : (k + 1) * lanes] for k in range(dcols // lanes)]

    def pair_of(got):
        pair = got.reshape(n_tp, n_fs, 2, r, lanes).transpose(2, 1, 0, 3, 4).reshape(2, width, lanes)
        return pair[0], pair[1]

    def down_of(got):
        down = got.reshape(n_tp, dcols // lanes, hid, lanes)
        return down.transpose(2, 0, 1, 3).reshape(hid, width)

    downs = jnp.concatenate([*in_lanes(d1), *in_lanes(d2)], axis=0)
    downs = gather_tp_beside(downs)
    mats, downs = lax.optimization_barrier((mats, downs))
    cut = dcols // lanes * hid
    first = (*pair_of(gather_tp(mats.reshape(-1, lanes))), down_of(downs[:, :cut]))
    down_second_served = down_of(downs[:, cut:])

    stream = prompt.astype(jnp.float32)
    normed = normed_of(stream)
    gate = jnp.dot(normed, first[0], preferred_element_type=jnp.float32)
    up = jnp.dot(normed, first[1], preferred_element_type=jnp.float32)
    hidden = (jax.nn.silu(gate) * up).astype(BF16)
    partial = jnp.dot(hidden, first[2], preferred_element_type=jnp.float32)
    tokens = prompt.shape[0] // n_fs
    own = lax.dynamic_slice_in_dim(prompt, lax.axis_index("fs") * tokens, tokens, 0).astype(jnp.float32)
    own = own + 0.5 * scatter_sum(partial)

    normed = spread_copies(normed_of(own), "tp", n_tp).reshape(n_tp * tokens, width)
    hidden = hidden_kernel(normed, whole, n_tp)
    step1, step2, step3, step4 = cast_in_plane(whole, rows)
    hidden = exchange(hidden, "tp")
    cast = step1()
    done = step2(cast)
    out = down_kernel(hidden, whole, hid)
    out = exchange(out.reshape(n_tp, tokens, dcols), "tp")
    cast = done()
    done = step3(cast)
    own = own + 0.5 * out.transpose(1, 0, 2).reshape(tokens, width)
    got = spread_far(own.astype(BF16))
    cast = done()
    done = step4(cast)
    gate_served, up_served = done()
    result = gather_near(got)
    return (result, first[0], first[1], first[2], gate_served, up_served, down_second_served)


def solution(mesh):
    return jax.shard_map(
        on_device,
        mesh=mesh,
        in_specs=(
            P(("grp", "tp"), None),
            P("fs"),
            P("fs", "tp"),
            P("fs", "tp"),
            P("fs", "tp"),
            P("fs"),
            P("fs", "tp"),
            P("fs", "tp"),
            P("fs", "tp"),
        ),
        out_specs=(
            P(("grp", "tp"), None),
            P("grp", "fs"),
            P("grp", "fs"),
            P("fs", "grp"),
            P("grp", "fs"),
            P("grp", "fs"),
            P("fs", "grp"),
        ),
        check_vma=False,
    )
```

```python
import jax
import jax.numpy as jnp
from jax import lax
from jax.experimental import pallas as pl
from jax.experimental.layout import Layout, with_layout_constraint
from jax.experimental.pallas import tpu as pltpu
from jax.sharding import PartitionSpec as P


EPS = 1e-06
NEAR = 4
BF16 = jnp.bfloat16


def fold(gain, weight):
    return (gain[:, None] * weight).astype(BF16)


def normed_of(stream):
    return (stream * lax.rsqrt(jnp.mean(stream * stream, axis=-1, keepdims=True) + EPS)).astype(BF16)


def row_major(array):
    return with_layout_constraint(array, Layout(major_to_minor=tuple(range(array.ndim))))


def exchange(blocks, axis, groups=None):
    return lax.all_to_all(blocks, axis, split_axis=0, concat_axis=0, tiled=True, axis_index_groups=groups)


def spread_copies(array, axis, members, groups=None):
    copies = jnp.broadcast_to(array, (members, *array.shape))
    if groups is not None and len(groups[0]) > members:
        copies = copies.reshape(len(groups[0]), *array.shape[1:])
    return exchange(copies, axis, groups)


def far_groups(n, stride=NEAR):
    return [list(range(i, n, stride)) for i in range(stride)]


def chip_groups(n):
    return [list(range(c, n, 2)) for c in range(2)]


def gather_tp(array):
    n = lax.axis_size("tp")
    mine = spread_copies(array, "tp", n // 2, chip_groups(n))
    other = lax.ppermute(mine, "tp", [(i, i ^ 1) for i in range(n)])
    even = lax.axis_index("tp") % 2 == 0
    both = jnp.stack([jnp.where(even, mine, other), jnp.where(even, other, mine)], axis=1)
    return both.reshape(n, *array.shape)


def shift_tp(array, steps):
    n = lax.axis_size("tp")
    return lax.ppermute(array, "tp", [(i, (i + steps) % n) for i in range(n)])


def gather_tp_beside(array):
    n = lax.axis_size("tp")
    chips = n // 2
    me = lax.axis_index("tp")
    mine = jnp.zeros((chips, *array.shape), array.dtype)
    for d in range(chips):
        piece = array if d == 0 else shift_tp(array, -2 * d)
        mine = lax.dynamic_update_index_in_dim(mine, piece, (me // 2 + d) % chips, 0)
    other = lax.ppermute(mine, "tp", [(i, i ^ 1) for i in range(n)])
    even = me % 2 == 0
    both = jnp.stack([jnp.where(even, mine, other), jnp.where(even, other, mine)], axis=1)
    return both.reshape(n, *array.shape)


def shift(array, steps):
    n = lax.axis_size("fs")
    return lax.ppermute(array, "fs", [(i, (i + steps) % n) for i in range(n)])


def part_of(blocks, index, axis=0):
    return lax.dynamic_index_in_dim(blocks, index % blocks.shape[axis], axis, keepdims=False)


def scatter_sum(partial):
    n = lax.axis_size("fs")
    me = lax.axis_index("fs")
    far = n // NEAR
    rows = partial.shape[0] // n
    width = partial.shape[1]
    f32 = jnp.float32

    blocks = partial.astype(BF16).reshape(far, NEAR, rows, width)
    keep, ahead, across, behind = (part_of(blocks, me + d, 1) for d in range(NEAR))
    h = far // 2
    ahead, behind = shift(ahead, 1), shift(behind, -1)
    low, high = shift(across[:h], 2), shift(across[h:], -2)
    total = keep.astype(f32) + ahead.astype(f32) + behind.astype(f32)
    total = total + jnp.concatenate([low, high], axis=0).astype(f32)

    blocks = total.astype(BF16).reshape(far // 2, 2, rows, width)
    side = me // NEAR
    keep, other = part_of(blocks, side, 1), part_of(blocks, side + 1, 1)
    h = far // 4
    low, high = shift(other[:h], NEAR), shift(other[h:], -NEAR)
    total = keep.astype(f32) + jnp.concatenate([low, high], axis=0).astype(f32)

    got = exchange(total.astype(BF16), "fs", far_groups(n, 2 * NEAR))
    return jnp.sum(got.astype(f32), axis=0)


def spread_far(own):
    n = lax.axis_size("fs")
    return spread_copies(own, "fs", n // NEAR, far_groups(n))


def gather_near(got):
    n = lax.axis_size("fs")
    me = lax.axis_index("fs")
    far, rows, width = got.shape
    h = far // 2
    ahead = shift(got, -1)
    behind = shift(got, 1)
    low, high = shift(got[:h], 2), shift(got[h:], -2)
    out = jnp.zeros((far, NEAR, rows, width), got.dtype)
    pieces = (got, ahead, jnp.concatenate([low, high], axis=0), behind)
    for d, piece in enumerate(pieces):
        out = lax.dynamic_update_index_in_dim(out, piece, (me + d) % NEAR, 1)
    return out.reshape(n * rows, width)


def cast_in_plane(whole, rows):
    n, n_tp = lax.axis_size("fs"), lax.axis_size("tp")
    chips = n_tp // 2
    per = n // n_tp
    me, t = lax.axis_index("fs"), lax.axis_index("tp")
    planes, _, cols = whole.shape
    lanes = cols * 2 // per
    home = me // per
    ahead = (t // 2 - home // 2) % chips

    def at(f, steps, core):
        return f * n_tp + 2 * ((f // per // 2 + steps) % chips) + core

    def hop(array, pairs):
        return lax.ppermute(array, ("fs", "tp"), [pair for f in range(n) for pair in pairs(f)])

    def first():
        half = me % per // 2 * rows
        both = [lax.dynamic_slice(whole, (0, 2 * m * rows + half, 0), (planes, rows, cols)) for m in range(2)]
        both = [jnp.where(me % 2 == 0, w[..., :lanes], w[..., lanes:]) for w in both]
        return jnp.stack([w.reshape(planes * rows, lanes) for w in both])

    def second(array):
        other = hop(array, lambda f: [(f * n_tp + f // per, f * n_tp + (f // per ^ 1))])
        return lambda: jnp.where(t == home, array, other)

    def third(array):
        up = hop(array, lambda f: [(at(f, 0, c), at(f, 1, c)) for c in range(2)])
        down = hop(array, lambda f: [(at(f, 0, c), at(f, -1, c)) for c in range(2)])
        return lambda: jnp.where(ahead == 0, array, jnp.where(ahead == 1, up, down))

    def fourth(array):
        gate = hop(array[0], lambda f: [(at(f, 1, c), at(f, 2, c)) for c in range(2)])
        up = hop(array[1], lambda f: [(at(f, -1, c), at(f, -2, c)) for c in range(2)])
        return lambda: (jnp.where(ahead == 2, gate, array[0]), jnp.where(ahead == 2, up, array[1]))

    return first, second, third, fourth


STEPS = 4


def hidden_kernel(normed, whole, copies):
    tokens, width = normed.shape
    planes, _, cols = whole.shape
    rows = width // planes
    halves = 2
    per = planes // STEPS
    group = 256 // rows

    def body(x_ref, w_ref, o_ref, acc_ref):
        step = pl.program_id(0)

        @pl.when(step == 0)
        def _():
            acc_ref[...] = jnp.zeros_like(acc_ref)

        for j in range(per // group):
            x = x_ref[:, j * group * rows : (j + 1) * group * rows]
            for m in range(2 * halves):
                w = jnp.concatenate(
                    [w_ref[j * group + k, m * rows : (m + 1) * rows, :] for k in range(group)], axis=0
                )
                acc_ref[m] += jnp.dot(x, w, preferred_element_type=jnp.float32)

        @pl.when(step == STEPS - 1)
        def _():
            for m in range(halves):
                gate, up = acc_ref[m], acc_ref[halves + m]
                value = (gate / (1.0 + jnp.exp(-gate)) * up).astype(BF16)
                for c in range(copies):
                    o_ref[c, :, m * cols : (m + 1) * cols] = value

    return pl.pallas_call(
        body,
        grid=(STEPS,),
        in_specs=[
            pl.BlockSpec((tokens, width // STEPS), lambda i: (0, i)),
            pl.BlockSpec((per, 2 * halves * rows, cols), lambda i: (i, 0, 0)),
        ],
        out_specs=pl.BlockSpec((copies, tokens, halves * cols), lambda i: (0, 0, 0)),
        out_shape=jax.ShapeDtypeStruct((copies, tokens, halves * cols), BF16),
        scratch_shapes=[pltpu.VMEM((2 * halves, tokens, cols), jnp.float32)],
        name="hidden_second",
    )(normed, whole)


def down_kernel(hidden, whole, hid):
    n_tp, tokens, cols = hidden.shape
    planes, rows, width = whole.shape
    per = planes // STEPS
    blocks = n_tp // STEPS
    each = per // blocks

    def body(h_ref, w_ref, o_ref):
        step = pl.program_id(0)

        @pl.when(step == 0)
        def _():
            o_ref[...] = jnp.zeros_like(o_ref)

        for b in range(blocks):
            w = w_ref[b * each : (b + 1) * each].reshape(cols, width)
            o_ref[...] += jnp.dot(h_ref[b], w, preferred_element_type=jnp.float32)

    return pl.pallas_call(
        body,
        grid=(STEPS,),
        in_specs=[
            pl.BlockSpec((blocks, tokens, cols), lambda i: (i, 0, 0)),
            pl.BlockSpec((per, hid, width), lambda i: (i, rows // hid - 1, 0)),
        ],
        out_specs=pl.BlockSpec((tokens, width), lambda i: (0, 0)),
        out_shape=jax.ShapeDtypeStruct((tokens, width), jnp.float32),
        name="down_second",
    )(hidden, whole)


def on_device(
    prompt,
    gain_first,
    gate_first,
    up_first,
    down_first,
    gain_second,
    gate_second,
    up_second,
    down_second,
):
    n_fs = lax.axis_size("fs")
    n_tp = lax.axis_size("tp")
    rows, cols = gate_first.shape
    hid, dcols = down_first.shape
    width = prompt.shape[1]
    half = cols // dcols

    g1, u1 = fold(gain_first, gate_first), fold(gain_first, up_first)
    g2, u2 = fold(gain_second, gate_second), fold(gain_second, up_second)
    d1, d2 = down_first.astype(BF16), down_second.astype(BF16)

    pack = [m[:, k * dcols : (k + 1) * dcols] for m in (g2, u2) for k in range(half)] + [d2]
    whole = lax.all_gather(row_major(jnp.concatenate(pack, axis=0)), "fs", axis=0, tiled=True)
    whole = row_major(whole).reshape(n_fs, 2 * half * rows + hid, dcols)

    r = rows // n_tp
    lanes = cols * n_tp // n_fs
    per = n_fs // n_tp
    mats = jnp.stack([g1, u1]).reshape(2, n_tp, r, cols).transpose(1, 0, 2, 3)
    mats = exchange(mats, "tp")
    mats = mats.reshape(n_tp, 2, r, per, lanes).transpose(0, 3, 1, 2, 4).reshape(n_fs, 2, r, lanes)
    mats, d1, d2 = lax.optimization_barrier((mats, d1, d2))
    mats = exchange(mats, "fs")

    def in_lanes(down):
        return [down[:, k * lanes : (k + 1) * lanes] for k in range(dcols // lanes)]

    def pair_of(got):
        pair = got.reshape(n_tp, n_fs, 2, r, lanes).transpose(2, 1, 0, 3, 4).reshape(2, width, lanes)
        return pair[0], pair[1]

    def down_of(got):
        down = got.reshape(n_tp, dcols // lanes, hid, lanes)
        return down.transpose(2, 0, 1, 3).reshape(hid, width)

    downs = jnp.concatenate([*in_lanes(d1), *in_lanes(d2)], axis=0)
    downs = gather_tp_beside(downs)
    mats, downs = lax.optimization_barrier((mats, downs))
    cut = dcols // lanes * hid
    first = (*pair_of(gather_tp(mats.reshape(-1, lanes))), down_of(downs[:, :cut]))
    down_second_served = down_of(downs[:, cut:])

    stream = prompt.astype(jnp.float32)
    normed = normed_of(stream)
    gate = jnp.dot(normed, first[0], preferred_element_type=jnp.float32)
    up = jnp.dot(normed, first[1], preferred_element_type=jnp.float32)
    hidden = (jax.nn.silu(gate) * up).astype(BF16)
    partial = jnp.dot(hidden, first[2], preferred_element_type=jnp.float32)
    tokens = prompt.shape[0] // n_fs
    own = lax.dynamic_slice_in_dim(prompt, lax.axis_index("fs") * tokens, tokens, 0).astype(jnp.float32)
    own = own + 0.5 * scatter_sum(partial)

    normed = spread_copies(normed_of(own), "tp", n_tp).reshape(n_tp * tokens, width)
    hidden = hidden_kernel(normed, whole, n_tp)
    step1, step2, step3, step4 = cast_in_plane(whole, rows)
    hidden = exchange(hidden, "tp")
    cast = step1()
    done = step2(cast)
    out = down_kernel(hidden, whole, hid)
    out = exchange(out.reshape(n_tp, tokens, dcols), "tp")
    cast = done()
    done = step3(cast)
    own = own + 0.5 * out.transpose(1, 0, 2).reshape(tokens, width)
    got = spread_far(own.astype(BF16))
    cast = done()
    done = step4(cast)
    gate_served, up_served = done()
    result = gather_near(got)
    return (result, first[0], first[1], first[2], gate_served, up_served, down_second_served)


def solution(mesh):
    return jax.shard_map(
        on_device,
        mesh=mesh,
        in_specs=(
            P(("grp", "tp"), None),
            P("fs"),
            P("fs", "tp"),
            P("fs", "tp"),
            P("fs", "tp"),
            P("fs"),
            P("fs", "tp"),
            P("fs", "tp"),
            P("fs", "tp"),
        ),
        out_specs=(
            P(("grp", "tp"), None),
            P("grp", "fs"),
            P("grp", "fs"),
            P("fs", "grp"),
            P("grp", "fs"),
            P("grp", "fs"),
            P("fs", "grp"),
        ),
        check_vma=False,
    )
```
